512 devices in a mesh: ep: 32 (over z, core), tp: 16 (over y, x).
Axes of the slice: x: 4, y: 4, z: 16, core: 2. Of those that a mesh axis runs over, the one named last changes fastest.
Arguments:
- token_rows: bfloat16 [768, 2048], P('ep', 'tp'), may hold values from -6 to 6
- prior_state: float32 [768, 64, 2048], P('ep', None, 'tp'), may hold values from -4 to 4
- first_gain: bfloat16 [2048], replicated, may hold values from 0.099609375 to 1.8984375
- w_recept: bfloat16 [2048, 2048], P(None, 'tp'), may hold values from -0.125 to 0.125
- w_key: bfloat16 [2048, 2048], P(None, 'tp'), may hold values from -0.125 to 0.125
- w_value: bfloat16 [2048, 2048], P(None, 'tp'), may hold values from -0.125 to 0.125
- decay_down: bfloat16 [2048, 96], P('tp'), may hold values from -0.125 to 0.125
- decay_up: bfloat16 [96, 2048], P(None, 'tp'), may hold values from -0.625 to 0.625
- decay_base: float32 [2048], P('tp'), may hold values from -4 to 3
- iclr_down: bfloat16 [2048, 96], P('tp'), may hold values from -0.125 to 0.125
- iclr_up: bfloat16 [96, 2048], P(None, 'tp'), may hold values from -0.625 to 0.625
- iclr_base: float32 [2048], P('tp'), may hold values from -4 to 4
- key_scale: bfloat16 [2048], P('tp'), may hold values from 0.29882812 to 1.5
- key_mix: bfloat16 [2048], P('tp'), may hold values from 0 to 2
- head_gain: bfloat16 [2048], P('tp'), may hold values from 0.099609375 to 1.8984375
- w_out: bfloat16 [2048, 2048], P(None, 'tp'), may hold values from -0.125 to 0.125
- second_gain: bfloat16 [2048], replicated, may hold values from 0.099609375 to 1.8984375
- routes: int32 [768, 4], P('ep'), may hold values from 0 to 31, all different within a row; in each aligned block of 24 rows (0 to 23, 24 to 47, ...) at most 4 rows name the same one
- route_weights: float32 [768, 4], P('ep'), may hold values from 0.2 to 1
- exp_gate: bfloat16 [32, 2048, 2048], P('ep', None, 'tp'), may hold values from -0.125 to 0.125
- exp_up: bfloat16 [32, 2048, 2048], P('ep', None, 'tp'), may hold values from -0.125 to 0.125
- exp_down: bfloat16 [32, 2048, 2048], P('ep', 'tp'), may hold values from -0.125 to 0.125
- dense_gate: bfloat16 [2048, 512], P(None, 'tp'), may hold values from -0.125 to 0.125
- dense_up: bfloat16 [2048, 512], P(None, 'tp'), may hold values from -0.125 to 0.125
- dense_down: bfloat16 [512, 2048], P('tp'), may hold values from -0.25 to 0.25
- dense_mix: bfloat16 [2048], replicated, may hold values from -0.125 to 0.125
Outputs:
- layer_out: bfloat16 [768, 2048], P('ep', 'tp')
- next_state: float32 [768, 64, 2048], P('ep', None, 'tp')
The draws below stay inside these ranges and needn't reach their ends.
Inputs may be any that keep to these rules, and one draw needn't show every extreme that they name: `routes`: each row names 4 different experts. Among the rows of one index of ep no expert is named by more than 4 rows, and in every draw some expert is named by exactly 4 of them.
All inputs are finite; a program needn't handle non-finite values.
Results may differ from the reference program's by a relative error of at most 0.018.
Values may be sent and summed in bfloat16 or wider, within the bound.
No kernel may reach another device: no remote copies, remote signals or barrier semaphores. Data moves between devices by JAX's collectives and lax.ppermute only.
A program may use at most 64 MiB of HBM per device.

```python
import math
import jax
import jax.numpy as jnp
import numpy as np
from jax import lax

HEADS = 32
HEAD = 64
D = 2048
LR = 96
FF = 2048
DFF = 512
EXPERTS = 32
TOPK = 4
SEQ = 24
CAP = 4
BATCH = 768
N_TP = 16


def shard_levels(key, extent, shards, least, top_value):
    def one(dim, shards_of):
        heights = jax.random.uniform(jax.random.fold_in(jax.random.fold_in(key, 6), dim), (shards_of,), jnp.float32, least / len(shards), top_value / len(shards))
        return jnp.repeat(jnp.exp(heights), extent[dim] // shards_of).reshape((-1,) + (1,) * (len(extent) - dim - 1))

    factor_of = one(*shards[0])
    for cut in shards[1:]:
        factor_of = factor_of * one(*cut)
    return factor_of


def routed_block(rng, own, number, rows, number_of, top, limit, lean):
    sequence = jax.random.permutation(rng, number_of)
    crowded, common = shares(number_of, rows * top, limit, lean, True), shares(number_of, rows * top, limit, lean, False)
    places = jnp.arange(number_of)

    def named(sizes, rotation):
        used = int((sizes > 0).sum())
        fixed = max(1, used // 4)
        shifted = fixed + (places - fixed + rotation * (used - fixed)) % max(1, number_of - fixed)
        return jnp.zeros((number_of,), jnp.int32).at[sequence[jnp.where(places < fixed, places, shifted)]].set(jnp.asarray(sizes, jnp.int32))

    sizes = jnp.where(number % 4 == 0, named(crowded, number // 4), named(common, number - number // 4 - 1))
    mixed = jax.random.permutation(jax.random.fold_in(own, 3), number_of)
    donor, taker = mixed[0:number_of // 2 * 2:2], mixed[1:number_of // 2 * 2:2]
    slack = jnp.minimum(sizes[donor] - 1, limit - sizes[taker]) // 2
    slack = jnp.where((donor == sequence[0]) | (taker == sequence[0]) | (sizes[taker] == 0), 0, jnp.maximum(slack, 0))
    shifted = jax.random.randint(jax.random.fold_in(own, 4), (number_of // 2,), 0, 1 << 20) % (slack + 1)
    sizes = sizes.at[donor].add(-shifted).at[taker].add(shifted)
    labels = jnp.searchsorted(jnp.cumsum(sizes), jnp.arange(rows * top), side="right").astype(jnp.int32)
    table = labels.reshape(top, rows).T
    table = table[jax.random.permutation(jax.random.fold_in(own, 1), rows)]
    rotation = jax.random.randint(jax.random.fold_in(own, 2), (rows, 1), 0, top)
    return jnp.take_along_axis(table, (jnp.arange(top)[None, :] + rotation) % top, axis=1)


def shares(count, total, limit, skew, full):
    loads = [(1 << 20) // math.isqrt(standing ** skew) + 1 for standing in range(1, count + 1)]
    largest = limit if full else min(limit, max(-(-total // count), total * loads[0] // sum(loads)))
    least = 1 if total - largest >= count - 1 else 0
    given, surplus = [largest] + [least] * (count - 1), total - largest - least * (count - 1)
    while surplus > 0:
        movable = [i for i in range(1, count) if given[i] < largest] or [i for i in range(1, count) if given[i] < limit]
        pool, budget = sum([loads[i] for i in movable]), surplus
        for i in movable:
            extra = min(limit - given[i], max(1, budget * loads[i] // pool), surplus)
            given[i] = given[i] + extra
            surplus = surplus - extra
    return np.array(given)


def scatter_about(rng, extent, width, reach, cuts=(), kind=jnp.bfloat16):
    drawn = width * jax.random.normal(rng, extent, jnp.float32)
    if cuts:
        drawn = drawn * shard_levels(rng, extent, cuts, -0.22, 0.18)
    return jnp.clip(drawn, -reach, reach).astype(kind)


def setup_inputs(seed: int = 0) -> dict:
    arg_keys = jax.random.split(jax.random.key(seed), 27)
    token_rows = scatter_about(arg_keys[0], (BATCH, D), 1.0, 6.0, ((0, 32), (1, 16)))
    prior_state = scatter_about(arg_keys[1], (BATCH, HEAD, D), 0.5, 4.0, ((0, 32), (2, 16)), jnp.float32)
    first_gain = jnp.clip(1.0 + 0.18 * jax.random.normal(arg_keys[2], (D,), jnp.float32), 0.099609375, 1.8984375).astype(jnp.bfloat16)
    w_recept = scatter_about(arg_keys[3], (D, D), D ** -0.5, 0.125, ((1, 16),))
    w_key = scatter_about(arg_keys[4], (D, D), D ** -0.5, 0.125, ((1, 16),))
    w_value = scatter_about(arg_keys[5], (D, D), D ** -0.5, 0.125, ((1, 16),))
    decay_down = scatter_about(arg_keys[6], (D, LR), D ** -0.5, 0.125, ((0, 16),))
    decay_up = scatter_about(arg_keys[7], (LR, D), LR ** -0.5, 0.625, ((1, 16),))
    decay_base = jnp.clip(-4.0 + 7.0 * jax.random.uniform(arg_keys[8], (D,), jnp.float32) ** shard_levels(arg_keys[8], (D,), ((0, 16),), -0.2, 0.2), -4.0, 3.0)
    iclr_down = scatter_about(arg_keys[9], (D, LR), D ** -0.5, 0.125, ((0, 16),))
    iclr_up = scatter_about(arg_keys[10], (LR, D), LR ** -0.5, 0.625, ((1, 16),))
    iclr_base = scatter_about(arg_keys[11], (D,), 1.0, 4.0, ((0, 16),), jnp.float32)
    key_scale = jnp.clip(0.29882812 + 1.2011719 * jax.random.uniform(arg_keys[12], (D,), jnp.float32) ** shard_levels(arg_keys[12], (D,), ((0, 16),), -0.2, 0.2), 0.29882812, 1.5).astype(jnp.bfloat16)
    key_mix = jnp.clip(2.0 * jax.random.uniform(arg_keys[13], (D,), jnp.float32) ** shard_levels(arg_keys[13], (D,), ((0, 16),), -0.2, 0.2), 0.0, 2.0).astype(jnp.bfloat16)
    head_gain = jnp.clip(1.0 + 0.18 * jax.random.normal(arg_keys[14], (D,), jnp.float32), 0.099609375, 1.8984375).astype(jnp.bfloat16)
    w_out = scatter_about(arg_keys[15], (D, D), D ** -0.5, 0.125, ((1, 16),))
    second_gain = jnp.clip(1.0 + 0.18 * jax.random.normal(arg_keys[16], (D,), jnp.float32), 0.099609375, 1.8984375).astype(jnp.bfloat16)
    routes_keys = jax.random.split(jax.random.fold_in(arg_keys[17], 1), BATCH // SEQ)
    routes_turns = jax.random.permutation(jax.random.fold_in(arg_keys[17], 3), BATCH // SEQ)
    routes = jax.vmap(lambda own, number: routed_block(jax.random.fold_in(arg_keys[17], 2), own, number, SEQ, EXPERTS, TOPK, CAP, 2))(routes_keys, routes_turns).reshape((BATCH, TOPK))
    route_weights = jnp.clip(0.2 + 0.8 * jax.random.uniform(arg_keys[18], (BATCH, TOPK), jnp.float32) ** shard_levels(arg_keys[18], (BATCH, TOPK), ((0, 32),), -0.2, 0.2), 0.2, 1.0)
    exp_gate = scatter_about(arg_keys[19], (EXPERTS, D, FF), D ** -0.5, 0.125, ((0, 32), (2, 16)))
    exp_up = scatter_about(arg_keys[20], (EXPERTS, D, FF), D ** -0.5, 0.125, ((0, 32), (2, 16)))
    exp_down = scatter_about(arg_keys[21], (EXPERTS, FF, D), FF ** -0.5, 0.125, ((0, 32), (1, 16)))
    dense_gate = scatter_about(arg_keys[22], (D, DFF), D ** -0.5, 0.125, ((1, 16),))
    dense_up = scatter_about(arg_keys[23], (D, DFF), D ** -0.5, 0.125, ((1, 16),))
    dense_down = scatter_about(arg_keys[24], (DFF, D), DFF ** -0.5, 0.25, ((0, 16),))
    dense_mix = scatter_about(arg_keys[25], (D,), D ** -0.5, 0.125)
    return dict(token_rows=token_rows, prior_state=prior_state, first_gain=first_gain, w_recept=w_recept, w_key=w_key, w_value=w_value, decay_down=decay_down, decay_up=decay_up, decay_base=decay_base, iclr_down=iclr_down, iclr_up=iclr_up, iclr_base=iclr_base, key_scale=key_scale, key_mix=key_mix, head_gain=head_gain, w_out=w_out, second_gain=second_gain, routes=routes, route_weights=route_weights, exp_gate=exp_gate, exp_up=exp_up, exp_down=exp_down, dense_gate=dense_gate, dense_up=dense_up, dense_down=dense_down, dense_mix=dense_mix)


def norm_rows(values, gain):
    floats = values.astype(jnp.float32)
    mean_square = lax.optimization_barrier(jnp.mean(floats * floats, axis=1, keepdims=True))
    return (floats * lax.rsqrt(mean_square + 1e-06) * gain.astype(jnp.float32)).astype(jnp.bfloat16)

def product(left, right):
    return jnp.dot(left, right, preferred_element_type=jnp.float32)

def group_slots(group_routes):
    flat_ids = group_routes.reshape(SEQ * TOPK)
    onehot = (flat_ids[:, None] == jnp.arange(EXPERTS, dtype=jnp.int32)[None, :]).astype(jnp.float32)
    earlier = (jnp.arange(SEQ * TOPK)[:, None] > jnp.arange(SEQ * TOPK)[None, :]).astype(jnp.float32)
    before = jnp.dot(earlier, onehot, precision=lax.Precision.HIGHEST)
    ranking = lax.optimization_barrier(jnp.sum(before * onehot, axis=1)).astype(jnp.int32)
    return flat_ids * CAP + ranking

def one_expert(operands):
    expert_rows, gate_mat, up_mat, down_mat = operands
    hidden = (jax.nn.silu(product(expert_rows, gate_mat)) * product(expert_rows, up_mat)).astype(jnp.bfloat16)
    block = FF // N_TP
    partial_value = jnp.einsum('rjf,jfd->rjd', hidden.reshape(-1, N_TP, block).astype(jnp.float32), down_mat.reshape(N_TP, block, D).astype(jnp.float32), precision=lax.Precision.HIGHEST).astype(jnp.bfloat16)
    partial_value = lax.optimization_barrier(partial_value)
    return lax.optimization_barrier(jnp.sum(partial_value.astype(jnp.float32), axis=1)).astype(jnp.bfloat16)

def reference(token_rows, prior_state, first_gain, w_recept, w_key, w_value, decay_down, decay_up, decay_base, iclr_down, iclr_up, iclr_base, key_scale, key_mix, head_gain, w_out, second_gain, routes, route_weights, exp_gate, exp_up, exp_down, dense_gate, dense_up, dense_down, dense_mix):
    first = norm_rows(token_rows, first_gain)
    recept = product(first, w_recept).astype(jnp.bfloat16)
    key_rows = product(first, w_key).astype(jnp.bfloat16)
    value_rows = product(first, w_value).astype(jnp.bfloat16)
    decay_act = jnp.tanh(product(first, decay_down)).astype(jnp.bfloat16)
    rate_act = product(first, iclr_down).astype(jnp.bfloat16)
    decay_rate = jnp.exp(-jnp.exp(-jax.nn.softplus(-(decay_base + product(decay_act, decay_up))) - 0.5))
    iclr_rate = jax.nn.sigmoid(iclr_base + product(rate_act, iclr_up))
    key_float = key_rows.astype(jnp.float32)
    scaled = (key_float * key_scale.astype(jnp.float32)).reshape(BATCH, HEADS, HEAD)
    removal = scaled * lax.rsqrt(lax.optimization_barrier(jnp.sum(scaled * scaled, axis=-1, keepdims=True)) + 1e-06)
    written = (key_float * (1.0 + (iclr_rate - 1.0) * key_mix.astype(jnp.float32))).reshape(BATCH, HEADS, HEAD)
    state_grid = prior_state.reshape(BATCH, HEAD, HEADS, HEAD)
    recall = lax.optimization_barrier(jnp.sum(state_grid * removal[:, None], axis=-1))
    scaled_removal = removal * iclr_rate.reshape(BATCH, HEADS, HEAD)
    value_cols = jnp.transpose(value_rows.astype(jnp.float32).reshape(BATCH, HEADS, HEAD), (0, 2, 1))
    state_grid = state_grid * decay_rate.reshape(BATCH, 1, HEADS, HEAD) - recall[..., None] * scaled_removal[:, None] + value_cols[..., None] * written[:, None]
    read = lax.optimization_barrier(jnp.sum(state_grid * recept.astype(jnp.float32).reshape(BATCH, 1, HEADS, HEAD), axis=-1))
    read = jnp.transpose(read, (0, 2, 1))
    centered = read - lax.optimization_barrier(jnp.mean(read, axis=-1, keepdims=True))
    variance = lax.optimization_barrier(jnp.mean(centered * centered, axis=-1, keepdims=True))
    head_out = centered * lax.rsqrt(variance + 0.00064) * head_gain.astype(jnp.float32).reshape(HEADS, HEAD)
    head_out = head_out.reshape(BATCH, D).astype(jnp.bfloat16)
    mixer_out = product(head_out, w_out).astype(jnp.bfloat16)
    residual = (token_rows.astype(jnp.float32) + mixer_out.astype(jnp.float32)).astype(jnp.bfloat16)
    second = norm_rows(residual, second_gain)
    groups = BATCH // SEQ
    token_of = jnp.repeat(jnp.arange(SEQ, dtype=jnp.int32), TOPK)
    slot_index = jax.vmap(group_slots)(routes.reshape(groups, SEQ, TOPK))

    def group_table(slots_one):
        return jnp.full((EXPERTS * CAP,), SEQ, jnp.int32).at[slots_one].set(token_of)
    slot_table = jax.vmap(group_table)(slot_index)
    padded = jnp.concatenate([second.reshape(groups, SEQ, D), jnp.zeros((groups, 1, D), jnp.bfloat16)], axis=1)

    def take_rows(source, indices):
        return jnp.take(source, indices, axis=0)
    buffers = jax.vmap(take_rows)(padded, slot_table)
    by_expert = jnp.transpose(buffers.reshape(groups, EXPERTS, CAP, D), (1, 0, 2, 3)).reshape(EXPERTS, groups * CAP, D)
    results = lax.map(one_expert, (by_expert, exp_gate, exp_up, exp_down))
    returned = jnp.transpose(results.reshape(EXPERTS, groups, CAP, D), (1, 0, 2, 3)).reshape(groups, EXPERTS * CAP, D)
    picked = jax.vmap(take_rows)(returned, slot_index).astype(jnp.float32)
    weighted = picked * route_weights.reshape(groups, SEQ * TOPK)[..., None]
    routed = lax.optimization_barrier(jnp.sum(weighted.reshape(groups, SEQ, TOPK, D), axis=2)).reshape(BATCH, D)
    dense_hidden = (jax.nn.silu(product(second, dense_gate)) * product(second, dense_up)).astype(jnp.bfloat16)
    dense_out = product(dense_hidden, dense_down)
    mix_gate = jax.nn.sigmoid(product(second, dense_mix[:, None])[:, 0])
    layer_out = (residual.astype(jnp.float32) + routed + mix_gate[:, None] * dense_out).astype(jnp.bfloat16)
    return (layer_out, state_grid.reshape(BATCH, HEAD, D))
```

```python
import jax
import jax.numpy as jnp
from jax import lax
from jax.experimental import pallas as pl
from jax.experimental.pallas import tpu as pltpu
from jax.sharding import PartitionSpec as P


HEAD = 64
f32 = jnp.float32
bf16 = jnp.bfloat16

norm_eps = 1e-06
head_eps = 0.00064
key_eps = 1e-06


def dot(a, b):
    return jnp.dot(a, b, preferred_element_type=f32)


def split_dot(a, b):
    high = a.astype(bf16)
    low = (a - high.astype(f32)).astype(bf16)
    return dot(high, b) + dot(low, b)


def call(kernel, outs, *args, **kwargs):
    params = pltpu.CompilerParams(vmem_limit_bytes=12 << 20)
    return pl.pallas_call(kernel, out_shape=outs, compiler_params=params, **kwargs)(*args)


def shape(dims, dtype):
    return jax.ShapeDtypeStruct(dims, dtype)


def head_sum(x):
    first = lax.broadcasted_iota(jnp.int32, x.shape, 1) < HEAD
    left = jnp.sum(jnp.where(first, x, 0.0), axis=1, keepdims=True)
    right = jnp.sum(jnp.where(first, 0.0, x), axis=1, keepdims=True)
    return jnp.where(first, left, right)


def same_head():
    rows = lax.broadcasted_iota(jnp.int32, (2 * HEAD, 2 * HEAD), 0) // HEAD
    cols = lax.broadcasted_iota(jnp.int32, (2 * HEAD, 2 * HEAD), 1) // HEAD
    return jnp.where(rows == cols, 1.0, 0.0).astype(bf16)


def own_channel():
    rows = lax.broadcasted_iota(jnp.int32, (HEAD, 2 * HEAD), 0)
    cols = lax.broadcasted_iota(jnp.int32, (HEAD, 2 * HEAD), 1) % HEAD
    return rows == cols


def dot_t(a, b):
    return lax.dot_general(a, b, (((1,), (1,)), ((), ())), preferred_element_type=f32)


def message_kernel(place, tokens, gain, decay_down, iclr_down, out):
    rows = lax.broadcasted_iota(jnp.int32, gain.shape, 0)
    own = jnp.sum(jnp.where(rows == place[0], gain[...].astype(f32), 0.0), axis=0, keepdims=True)
    scaled = (tokens[...].astype(f32) * own).astype(bf16)
    count, seqs, width = out.shape
    rank = decay_down.shape[0]
    pad = jnp.zeros((seqs, width // 3 - rank), f32)
    whole = jnp.concatenate(
        [
            tokens[...].astype(f32),
            dot_t(scaled, decay_down[...]),
            pad,
            dot_t(scaled, iclr_down[...]),
            pad,
        ],
        axis=1,
    ).astype(bf16)
    for p in range(count):
        out[p] = whole


def slot_table(routes, slots):
    top, seqs = routes.shape
    expert = lax.broadcasted_iota(jnp.int32, (slots, seqs), 0) // 4
    matches = [routes[k : k + 1, :] == expert for k in range(top)]
    chosen = jnp.where(matches[0], 1.0, 0.0)
    for match in matches[1:]:
        chosen = chosen + jnp.where(match, 1.0, 0.0)
    earlier = lax.broadcasted_iota(jnp.int32, (seqs, seqs), 0) < lax.broadcasted_iota(
        jnp.int32, (seqs, seqs), 1
    )
    before = dot(chosen.astype(bf16), jnp.where(earlier, 1.0, 0.0).astype(bf16))
    place = (lax.broadcasted_iota(jnp.int32, (slots, seqs), 0) % 4).astype(f32)
    return matches, jnp.where(before == place, chosen, 0.0)


def routing_kernel(routes, hit_out):
    _, hit = slot_table(routes, hit_out.shape[0])
    hit_out[...] = hit.astype(bf16)


def weights_kernel(routes, weights, out):
    matches, hit = slot_table(routes, out.shape[0])
    total = jnp.zeros(out.shape, f32)
    for k, match in enumerate(matches):
        total = total + jnp.where(match, weights[k : k + 1, :], 0.0)
    out[...] = total * hit


def mixer_in_kernel(
    arrived,
    state,
    gain,
    w_recept,
    w_key,
    w_value,
    decay_up,
    decay_base,
    iclr_up,
    iclr_base,
    key_scale,
    key_mix,
    head_gain,
    heads_out,
    vectors_out,
):
    count, seqs, width = arrived.shape
    piece = width // 3
    rank = decay_up.shape[0]
    tokens = [arrived[p, :, :piece].astype(f32) for p in range(count)]
    squares = tokens[0] * tokens[0]
    for x in tokens[1:]:
        squares = squares + x * x
    scale = lax.rsqrt(
        jnp.sum(squares, axis=1, keepdims=True) * (1.0 / (count * piece)) + norm_eps
    )
    first = jnp.concatenate(
        [
            (x * scale * gain[p : p + 1, :].astype(f32)).astype(bf16)
            for p, x in enumerate(tokens)
        ],
        axis=1,
    )
    low = arrived[0, :, piece:].astype(f32)
    for p in range(1, count):
        low = low + arrived[p, :, piece:].astype(f32)
    low = low * scale
    decay_act = jnp.tanh(low[:, :rank]).astype(bf16)
    rate_act = low[:, piece : piece + rank].astype(bf16)
    recept = dot(first, w_recept[...]).astype(bf16).astype(f32)
    key = dot(first, w_key[...]).astype(bf16).astype(f32)
    value = dot(first, w_value[...]).astype(bf16).astype(f32)
    decay_pre = -(decay_base[...] + dot(decay_act, decay_up[...]))
    softplus = jnp.maximum(decay_pre, 0.0) + jnp.log1p(jnp.exp(-jnp.abs(decay_pre)))
    decay = jnp.exp(-jnp.exp(-softplus - 0.5))
    rate = jax.nn.sigmoid(iclr_base[...] + dot(rate_act, iclr_up[...]))
    scaled = key * key_scale[...].astype(f32)
    removal = scaled * lax.rsqrt(head_sum(scaled * scaled) + key_eps)
    written = key * (1.0 + (rate - 1.0) * key_mix[...].astype(f32))
    scaled_removal = removal * rate
    together = same_head()
    own = own_channel()

    def against(weights):
        grid = state[...] * weights[:, None, :]
        spread = split_dot(grid.reshape(seqs * HEAD, piece), together)
        return jnp.sum(jnp.where(own, spread.reshape(seqs, HEAD, piece), 0.0), axis=1)

    recall = against(removal)
    read = (
        against(decay * recept)
        - recall * head_sum(scaled_removal * recept)
        + value * head_sum(written * recept)
    )
    centered = read - head_sum(read) * (1.0 / HEAD)
    variance = head_sum(centered * centered) * (1.0 / HEAD)
    head_out = (centered * lax.rsqrt(variance + head_eps) * head_gain[...].astype(f32)).astype(bf16)
    for p in range(count):
        heads_out[p] = head_out
    for i, v in enumerate((removal, decay, scaled_removal, value, written)):
        vectors_out[i] = v


def state_kernel(state, vectors, out):
    seqs, _, width = state.shape
    removal, decay, scaled_removal, value, written = (
        vectors[i][:, None, :] for i in range(5)
    )
    together = same_head()
    grid = state[...]
    recall = split_dot((grid * removal).reshape(seqs * HEAD, width), together)
    spread = jnp.where(own_channel(), value, 0.0).astype(bf16).reshape(seqs * HEAD, width)
    values = dot(spread, together)
    out[...] = (
        grid * decay
        - recall.reshape(seqs, HEAD, width) * scaled_removal
        + values.reshape(seqs, HEAD, width) * written
    )


def dispatch_kernel(heads, w_out, tokens, hit, residual_out, outgoing):
    count = heads.shape[0]
    rows = jnp.concatenate([heads[p] for p in range(count)], axis=1)
    mixed = dot(rows, w_out[...]).astype(bf16).astype(f32)
    residual = (tokens[...].astype(f32) + mixed).astype(bf16)
    residual_out[...] = residual
    outgoing[...] = dot(hit[...], residual).astype(bf16)


def spread_kernel(arrived, residual, out):
    slots = arrived.shape[0]
    for p in range(out.shape[0]):
        out[p, :slots] = arrived[...]
        out[p, slots:] = residual[...]


def expert_kernel(
    arrived, gain, gate, up, down, dense_gate, dense_up, dense_down, out, dense_rows_out
):
    count, rows, piece = arrived.shape
    slots = rows - dense_rows_out.shape[0]
    pieces = [arrived[p].astype(f32) for p in range(count)]
    squares = pieces[0] * pieces[0]
    for x in pieces[1:]:
        squares = squares + x * x
    scale = lax.rsqrt(
        jnp.sum(squares, axis=1, keepdims=True) * (1.0 / (count * piece)) + norm_eps
    )
    normed = [
        (x * scale * gain[p : p + 1, :].astype(f32)).astype(bf16) for p, x in enumerate(pieces)
    ]
    second = jnp.concatenate(normed, axis=1)
    routed, dense = second[:slots], second[slots:]
    hidden = (jax.nn.silu(dot(routed, gate[...])) * dot(routed, up[...])).astype(bf16)
    dense_hidden = (
        jax.nn.silu(dot_t(dense, dense_gate[...])) * dot_t(dense, dense_up[...])
    ).astype(bf16)
    for p in range(count):
        cols = slice(p * piece, (p + 1) * piece)
        out[p, :slots] = dot(hidden, down[:, cols]).astype(bf16)
        out[p, slots:] = dot(dense_hidden, dense_down[:, cols]).astype(bf16)
    dense_rows_out[...] = dense


def mix_kernel(rows, weights, out):
    count, width = weights.shape
    mix = jnp.zeros(out.shape, f32)
    for p in range(count):
        mix = mix + rows[:, p * width : (p + 1) * width].astype(f32) * weights[
            p : p + 1, :
        ].astype(f32)
    mix = jax.nn.sigmoid(jnp.sum(mix, axis=1, keepdims=True))
    out[...] = jnp.broadcast_to(mix, out.shape)


def total_kernel(partial, expert_out, dense_out):
    count = partial.shape[0]
    slots = expert_out.shape[0]
    total = partial[0].astype(f32)
    for p in range(1, count):
        total = total + partial[p].astype(f32)
    expert_out[...] = total[:slots].astype(bf16)
    dense_out[...] = total[slots:]


def base_kernel(residual, mix, dense, out):
    out[...] = residual[...].astype(f32) + mix[...] * dense[...]


def final_kernel(returned, weights, base, out):
    high = weights[...].astype(bf16)
    rest = weights[...] - high.astype(f32)
    middle = rest.astype(bf16)
    low = (rest - middle.astype(f32)).astype(bf16)
    values = returned[...]
    total = base[...]
    for part in (low, middle, high):
        total = total + lax.dot_general(
            part, values, (((0,), (0,)), ((), ())), preferred_element_type=f32
        )
    out[...] = total.astype(bf16)


def exchange(value, axis):
    return lax.all_to_all(value, axis, 0, 0, tiled=True)


def near(dims, dtype):
    return pltpu.VMEM(dims, dtype)


def held(*values):
    return [pltpu.with_memory_space_constraint(v, pltpu.VMEM) for v in values]


def local(
    token_rows,
    prior_state,
    first_gain,
    w_recept,
    w_key,
    w_value,
    decay_down,
    decay_up,
    decay_base,
    iclr_down,
    iclr_up,
    iclr_base,
    key_scale,
    key_mix,
    head_gain,
    w_out,
    second_gain,
    routes,
    route_weights,
    exp_gate,
    exp_up,
    exp_down,
    dense_gate,
    dense_up,
    dense_down,
    dense_mix,
):
    seqs, width = token_rows.shape
    count = lax.axis_size("tp")
    groups = lax.axis_size("ep")
    slots = groups * 4
    rows = slots + seqs
    place = lax.axis_index("tp").reshape(1).astype(jnp.int32)
    row = lambda v: v.reshape(1, width)
    pieces = lambda v: v.reshape(count, width)
    in_smem = pl.BlockSpec(memory_space=pltpu.SMEM)
    in_vmem = pl.BlockSpec(memory_space=pltpu.VMEM)
    message = call(
        message_kernel,
        near((count, seqs, 3 * width), bf16),
        place,
        *held(token_rows, pieces(first_gain), decay_down.T, iclr_down.T),
        in_specs=[in_smem] + [in_vmem] * 4,
    )
    arrived = exchange(message, "tp")
    hit = call(routing_kernel, near((slots, seqs), bf16), *held(routes.T))
    heads, vectors = call(
        mixer_in_kernel,
        (near((count, seqs, width), bf16), near((5, seqs, width), f32)),
        *held(
            arrived,
            prior_state,
            pieces(first_gain),
            w_recept,
            w_key,
            w_value,
            decay_up,
            row(decay_base),
            iclr_up,
            row(iclr_base),
            row(key_scale),
            row(key_mix),
            row(head_gain),
        ),
    )
    heads_all = exchange(heads, "tp")
    block = 8
    next_state = call(
        state_kernel,
        shape(prior_state.shape, f32),
        prior_state,
        vectors,
        grid=(seqs // block,),
        in_specs=[
            pl.BlockSpec((block, HEAD, width), lambda i: (i, 0, 0)),
            pl.BlockSpec((5, block, width), lambda i: (0, i, 0)),
        ],
        out_specs=pl.BlockSpec((block, HEAD, width), lambda i: (i, 0, 0)),
    )
    residual, outgoing = call(
        dispatch_kernel,
        (near((seqs, width), bf16), shape((slots, width), bf16)),
        *held(heads_all, w_out, token_rows, hit),
    )
    sent = exchange(outgoing.reshape(groups, 4, width), "ep").reshape(slots, width)
    slot_weights = call(weights_kernel, near((slots, seqs), f32), *held(routes.T, route_weights.T))
    gathered = exchange(
        call(spread_kernel, shape((count, rows, width), bf16), *held(sent, residual)), "tp"
    )
    partial, dense_rows = call(
        expert_kernel,
        (shape((count, rows, width), bf16), near((seqs, count * width), bf16)),
        *held(
            gathered,
            pieces(second_gain),
            exp_gate[0],
            exp_up[0],
            exp_down[0],
            dense_gate.T,
            dense_up.T,
            dense_down,
        ),
    )
    mix = call(mix_kernel, near((seqs, width), f32), *held(dense_rows, pieces(dense_mix)))
    expert_out, dense_out = call(
        total_kernel,
        (shape((slots, width), bf16), near((seqs, width), f32)),
        *held(exchange(partial, "tp")),
    )
    base = call(base_kernel, near((seqs, width), f32), *held(residual, mix, dense_out))
    returned = exchange(expert_out.reshape(groups, 4, width), "ep")
    layer_out = call(
        final_kernel,
        shape((seqs, width), bf16),
        *held(returned.reshape(slots, width), slot_weights, base),
    )
    return (layer_out, next_state)


def solution(mesh):
    in_specs = (
        P("ep", "tp"),
        P("ep", None, "tp"),
        P(),
        P(None, "tp"),
        P(None, "tp"),
        P(None, "tp"),
        P("tp", None),
        P(None, "tp"),
        P("tp"),
        P("tp", None),
        P(None, "tp"),
        P("tp"),
        P("tp"),
        P("tp"),
        P("tp"),
        P(None, "tp"),
        P(),
        P("ep", None),
        P("ep", None),
        P("ep", None, "tp"),
        P("ep", None, "tp"),
        P("ep", "tp", None),
        P(None, "tp"),
        P(None, "tp"),
        P("tp", None),
        P(),
    )
    out_specs = (P("ep", "tp"), P("ep", None, "tp"))
    return jax.shard_map(local, mesh=mesh, in_specs=in_specs, out_specs=out_specs, check_vma=False)
```

```python
import jax
import jax.numpy as jnp
from jax import lax
from jax.experimental import pallas as pl
from jax.experimental.pallas import tpu as pltpu
from jax.sharding import PartitionSpec as P


HEAD = 64
f32 = jnp.float32
bf16 = jnp.bfloat16

FIRST = {"tp": 10, "ep": 17}

norm_eps = 1e-06
head_eps = 0.00064
key_eps = 1e-06


def dot(a, b):
    return jnp.dot(a, b, preferred_element_type=f32)


def split_dot(a, b):
    high = a.astype(bf16)
    low = (a - high.astype(f32)).astype(bf16)
    return dot(high, b) + dot(low, b)


def call(kernel, outs, *args, **kwargs):
    params = pltpu.CompilerParams(vmem_limit_bytes=12 << 20)
    return pl.pallas_call(
        kernel, out_shape=outs, compiler_params=params, **kwargs
    )(*args)


def shape(dims, dtype):
    return jax.ShapeDtypeStruct(dims, dtype)


def head_sum(x):
    first = lax.broadcasted_iota(jnp.int32, x.shape, 1) < HEAD
    left = jnp.sum(jnp.where(first, x, 0.0), axis=1, keepdims=True)
    right = jnp.sum(jnp.where(first, 0.0, x), axis=1, keepdims=True)
    return jnp.where(first, left, right)


def same_head():
    rows = lax.broadcasted_iota(jnp.int32, (2 * HEAD, 2 * HEAD), 0) // HEAD
    cols = lax.broadcasted_iota(jnp.int32, (2 * HEAD, 2 * HEAD), 1) // HEAD
    return jnp.where(rows == cols, 1.0, 0.0).astype(bf16)


def own_channel():
    rows = lax.broadcasted_iota(jnp.int32, (HEAD, 2 * HEAD), 0)
    cols = lax.broadcasted_iota(jnp.int32, (HEAD, 2 * HEAD), 1) % HEAD
    return rows == cols


def dot_t(a, b):
    return lax.dot_general(a, b, (((1,), (1,)), ((), ())), preferred_element_type=f32)


def message_kernel(place, tokens, gain, decay_down, iclr_down, out):
    rows = lax.broadcasted_iota(jnp.int32, gain.shape, 0)
    own = jnp.sum(jnp.where(rows == place[0], gain[...].astype(f32), 0.0), axis=0, keepdims=True)
    scaled = (tokens[...].astype(f32) * own).astype(bf16)
    count, seqs, width = out.shape
    rank = decay_down.shape[0]
    pad = jnp.zeros((seqs, width // 3 - rank), f32)
    whole = jnp.concatenate(
        [
            tokens[...].astype(f32),
            dot_t(scaled, decay_down[...]),
            pad,
            dot_t(scaled, iclr_down[...]),
            pad,
        ],
        axis=1,
    ).astype(bf16)
    for p in range(count):
        out[p] = whole


def slot_table(routes, slots):
    top, seqs = routes.shape
    expert = (lax.broadcasted_iota(jnp.int32, (slots, seqs), 0) // 4 + FIRST["ep"]) % (slots // 4)
    matches = [routes[k : k + 1, :] == expert for k in range(top)]
    chosen = jnp.where(matches[0], 1.0, 0.0)
    for match in matches[1:]:
        chosen = chosen + jnp.where(match, 1.0, 0.0)
    earlier = lax.broadcasted_iota(jnp.int32, (seqs, seqs), 0) < lax.broadcasted_iota(
        jnp.int32, (seqs, seqs), 1
    )
    before = dot(chosen.astype(bf16), jnp.where(earlier, 1.0, 0.0).astype(bf16))
    place = (lax.broadcasted_iota(jnp.int32, (slots, seqs), 0) % 4).astype(f32)
    return matches, jnp.where(before == place, chosen, 0.0)


def prep_kernel(
    w_recept,
    w_key,
    w_value,
    decay_up,
    iclr_up,
    state,
    routes,
    gain,
    decay_base,
    iclr_base,
    key_scale,
    key_mix,
    head_gain,
    weights_out,
    ups_out,
    state_out,
    hit_out,
    gain_out,
    rows_out,
    sems,
):
    moves = [(w, weights_out.at[i]) for i, w in enumerate((w_recept, w_key, w_value))]
    moves += [(decay_up, ups_out.at[0]), (iclr_up, ups_out.at[1]), (state, state_out)]
    copies = [pltpu.make_async_copy(a, b, sems.at[i]) for i, (a, b) in enumerate(moves)]
    for copy in copies:
        copy.start()
    _, hit = slot_table(routes, hit_out.shape[0])
    hit_out[...] = hit.astype(bf16)
    gain_out[...] = gain[...].astype(f32)
    for i, row in enumerate((decay_base, iclr_base, key_scale, key_mix, head_gain)):
        rows_out[i : i + 1, :] = row[...].astype(f32)
    for copy in copies:
        copy.wait()


def weights_kernel(routes, weights, gain, out, gain_out):
    gain_out[...] = gain[...].astype(f32)
    matches, hit = slot_table(routes, out.shape[0])
    total = jnp.zeros(out.shape, f32)
    for k, match in enumerate(matches):
        total = total + jnp.where(match, weights[k : k + 1, :], 0.0)
    out[...] = total * hit


def mixer_in_kernel(
    arrived, state, gain, weights, ups, rows, heads_out, vectors_out
):
    count, seqs, width = arrived.shape
    piece = width // 3
    rank = ups.shape[1]
    decay_base, iclr_base, key_scale, key_mix, head_gain = (rows[i : i + 1, :] for i in range(5))
    tokens = [x[:, :piece].astype(f32) for x in by_feature(arrived, count)]
    squares = tokens[0] * tokens[0]
    for x in tokens[1:]:
        squares = squares + x * x
    scale = lax.rsqrt(
        jnp.sum(squares, axis=1, keepdims=True) * (1.0 / (count * piece)) + norm_eps
    )
    first = jnp.concatenate(
        [
            (x * scale * gain[p : p + 1, :]).astype(bf16)
            for p, x in enumerate(tokens)
        ],
        axis=1,
    )
    low = arrived[0, :, piece:].astype(f32)
    for p in range(1, count):
        low = low + arrived[p, :, piece:].astype(f32)
    low = low * scale
    decay_act = jnp.tanh(low[:, :rank]).astype(bf16)
    rate_act = low[:, piece : piece + rank].astype(bf16)
    recept = dot(first, weights[0]).astype(bf16).astype(f32)
    key = dot(first, weights[1]).astype(bf16).astype(f32)
    value = dot(first, weights[2]).astype(bf16).astype(f32)
    decay_pre = -(decay_base + dot(decay_act, ups[0]))
    softplus = jnp.maximum(decay_pre, 0.0) + jnp.log1p(jnp.exp(-jnp.abs(decay_pre)))
    decay = jnp.exp(-jnp.exp(-softplus - 0.5))
    rate = jax.nn.sigmoid(iclr_base + dot(rate_act, ups[1]))
    scaled = key * key_scale
    removal = scaled * lax.rsqrt(head_sum(scaled * scaled) + key_eps)
    written = key * (1.0 + (rate - 1.0) * key_mix)
    scaled_removal = removal * rate
    together = same_head()
    own = own_channel()

    def against(weights):
        grid = state[...] * weights[:, None, :]
        spread = split_dot(grid.reshape(seqs * HEAD, piece), together)
        return jnp.sum(jnp.where(own, spread.reshape(seqs, HEAD, piece), 0.0), axis=1)

    recall = against(removal)
    read = (
        against(decay * recept)
        - recall * head_sum(scaled_removal * recept)
        + value * head_sum(written * recept)
    )
    centered = read - head_sum(read) * (1.0 / HEAD)
    variance = head_sum(centered * centered) * (1.0 / HEAD)
    head_out = (centered * lax.rsqrt(variance + head_eps) * head_gain).astype(bf16)
    for p in range(count):
        heads_out[p] = head_out
    for i, v in enumerate((removal, decay, scaled_removal, value, written)):
        vectors_out[i] = v


def state_kernel(state, vectors, out):
    seqs, _, width = state.shape
    removal, decay, scaled_removal, value, written = (
        vectors[i][:, None, :] for i in range(5)
    )
    together = same_head()
    grid = state[...]
    recall = split_dot((grid * removal).reshape(seqs * HEAD, width), together)
    spread = jnp.where(own_channel(), value, 0.0).astype(bf16).reshape(seqs * HEAD, width)
    values = dot(spread, together)
    out[...] = (
        grid * decay
        - recall.reshape(seqs, HEAD, width) * scaled_removal
        + values.reshape(seqs, HEAD, width) * written
    )


def dispatch_kernel(heads, w_out, tokens, hit, residual_out, outgoing):
    count = heads.shape[0]
    rows = jnp.concatenate([x[...] for x in by_feature(heads, count)], axis=1)
    mixed = dot(rows, w_out[...]).astype(bf16).astype(f32)
    residual = (tokens[...].astype(f32) + mixed).astype(bf16)
    residual_out[...] = residual
    outgoing[...] = dot(hit[...], residual).astype(bf16)


def spread_kernel(arrived, residual, out):
    slots = arrived.shape[0]
    for p in range(out.shape[0]):
        out[p, :slots] = arrived[...]
        out[p, slots:] = residual[...]


def expert_kernel(
    arrived, gain, gate, up, down, dense_gate, dense_up, dense_down, out, dense_rows_out
):
    count, rows, piece = arrived.shape
    slots = rows - dense_rows_out.shape[0]
    pieces = [x[...].astype(f32) for x in by_feature(arrived, count)]
    squares = pieces[0] * pieces[0]
    for x in pieces[1:]:
        squares = squares + x * x
    scale = lax.rsqrt(
        jnp.sum(squares, axis=1, keepdims=True) * (1.0 / (count * piece)) + norm_eps
    )
    normed = [
        (x * scale * gain[p : p + 1, :]).astype(bf16) for p, x in enumerate(pieces)
    ]
    second = jnp.concatenate(normed, axis=1)
    routed, dense = second[:slots], second[slots:]
    hidden = (jax.nn.silu(dot(routed, gate[...])) * dot(routed, up[...])).astype(bf16)
    dense_hidden = (
        jax.nn.silu(dot_t(dense, dense_gate[...])) * dot_t(dense, dense_up[...])
    ).astype(bf16)
    for p, t in enumerate(member_order(count, "tp")):
        cols = slice(t * piece, (t + 1) * piece)
        out[p, :slots] = dot(hidden, down[:, cols]).astype(bf16)
        out[p, slots:] = dot(dense_hidden, dense_down[:, cols]).astype(bf16)
    dense_rows_out[...] = dense


def mix_kernel(rows, weights, out):
    count, width = weights.shape
    mix = jnp.zeros(out.shape, f32)
    for p in range(count):
        mix = mix + rows[:, p * width : (p + 1) * width].astype(f32) * weights[
            p : p + 1, :
        ].astype(f32)
    mix = jax.nn.sigmoid(jnp.sum(mix, axis=1, keepdims=True))
    out[...] = jnp.broadcast_to(mix, out.shape)


def total_kernel(partial, expert_out, dense_out):
    count = partial.shape[0]
    slots = expert_out.shape[0]
    total = partial[0].astype(f32)
    for p in range(1, count):
        total = total + partial[p].astype(f32)
    expert_out[...] = total[:slots].astype(bf16)
    dense_out[...] = total[slots:]


def base_kernel(residual, mix, dense, out):
    out[...] = residual[...].astype(f32) + mix[...] * dense[...]


def final_kernel(returned, weights, base, out):
    high = weights[...].astype(bf16)
    rest = weights[...] - high.astype(f32)
    middle = rest.astype(bf16)
    low = (rest - middle.astype(f32)).astype(bf16)
    values = returned[...]
    total = base[...]
    for part in (low, middle, high):
        total = total + lax.dot_general(
            part, values, (((0,), (0,)), ((), ())), preferred_element_type=f32
        )
    out[...] = total.astype(bf16)


def member_order(count, axis):
    return [(i + FIRST[axis]) % count for i in range(count)]


def by_feature(ref, count):
    return [ref.at[(t - FIRST["tp"]) % count] for t in range(count)]


def exchange(value, axis):
    order = member_order(lax.axis_size(axis), axis)
    return lax.all_to_all(value, axis, 0, 0, tiled=True, axis_index_groups=[order])


def near(dims, dtype):
    return pltpu.VMEM(dims, dtype)


def far(*values):
    return [pltpu.with_memory_space_constraint(v, pltpu.HBM) for v in values]


def held(*values):
    return [pltpu.with_memory_space_constraint(v, pltpu.VMEM) for v in values]


def local(
    token_rows,
    prior_state,
    first_gain,
    w_recept,
    w_key,
    w_value,
    decay_down,
    decay_up,
    decay_base,
    iclr_down,
    iclr_up,
    iclr_base,
    key_scale,
    key_mix,
    head_gain,
    w_out,
    second_gain,
    routes,
    route_weights,
    exp_gate,
    exp_up,
    exp_down,
    dense_gate,
    dense_up,
    dense_down,
    dense_mix,
):
    seqs, width = token_rows.shape
    count = lax.axis_size("tp")
    groups = lax.axis_size("ep")
    slots = groups * 4
    rows = slots + seqs
    place = lax.axis_index("tp").reshape(1).astype(jnp.int32)
    row = lambda v: v.reshape(1, width)
    pieces = lambda v: v.reshape(count, width)
    in_smem = pl.BlockSpec(memory_space=pltpu.SMEM)
    in_vmem = pl.BlockSpec(memory_space=pltpu.VMEM)
    message = call(
        message_kernel,
        shape((count, seqs, 3 * width), bf16),
        place,
        *far(token_rows, pieces(first_gain), decay_down.T, iclr_down.T),
        in_specs=[in_smem] + [in_vmem] * 4,
    )
    arrived = exchange(message, "tp")
    weights, ups, state, hit, gain, rows_of = call(
        prep_kernel,
        (
            near((3, *w_key.shape), bf16),
            near((2, *decay_up.shape), bf16),
            near(prior_state.shape, f32),
            near((slots, seqs), bf16),
            near((count, width), f32),
            near((8, width), f32),
        ),
        *far(
            w_recept,
            w_key,
            w_value,
            decay_up,
            iclr_up,
            prior_state,
            routes.T,
            pieces(first_gain),
            row(decay_base),
            row(iclr_base),
            row(key_scale),
            row(key_mix),
            row(head_gain),
        ),
        in_specs=[pl.BlockSpec(memory_space=pl.ANY)] * 6 + [in_vmem] * 7,
        scratch_shapes=[pltpu.SemaphoreType.DMA((6,))],
    )
    heads, vectors = call(
        mixer_in_kernel,
        (near((count, seqs, width), bf16), near((5, seqs, width), f32)),
        *held(arrived, state, gain, weights, ups, rows_of),
    )
    heads_all = exchange(heads, "tp")
    block = 8
    next_state = call(
        state_kernel,
        shape(prior_state.shape, f32),
        *far(prior_state),
        *held(vectors),
        grid=(seqs // block,),
        in_specs=[
            pl.BlockSpec((block, HEAD, width), lambda i: (i, 0, 0)),
            pl.BlockSpec((5, block, width), lambda i: (0, i, 0)),
        ],
        out_specs=pl.BlockSpec((block, HEAD, width), lambda i: (i, 0, 0)),
    )
    residual, outgoing = call(
        dispatch_kernel,
        (near((seqs, width), bf16), shape((slots, width), bf16)),
        *held(heads_all, w_out, token_rows, hit),
    )
    sent = exchange(outgoing.reshape(groups, 4, width), "ep").reshape(slots, width)
    slot_weights, second_scale = call(
        weights_kernel,
        (near((slots, seqs), f32), near((count, width), f32)),
        *far(routes.T, route_weights.T, pieces(second_gain)),
    )
    gathered = exchange(
        call(spread_kernel, shape((count, rows, width), bf16), *held(sent, residual)),
        "tp",
    )
    partial, dense_rows = call(
        expert_kernel,
        (shape((count, rows, width), bf16), near((seqs, count * width), bf16)),
        *held(
            gathered,
            second_scale,
            exp_gate[0],
            exp_up[0],
            exp_down[0],
            dense_gate.T,
            dense_up.T,
            dense_down,
        ),
    )
    mix = call(
        mix_kernel, near((seqs, width), f32), *held(dense_rows), *far(pieces(dense_mix))
    )
    expert_out, dense_out = call(
        total_kernel,
        (shape((slots, width), bf16), near((seqs, width), f32)),
        *held(exchange(partial, "tp")),
    )
    base = call(base_kernel, near((seqs, width), f32), *held(residual, mix, dense_out))
    returned = exchange(expert_out.reshape(groups, 4, width), "ep")
    layer_out = call(
        final_kernel,
        shape((seqs, width), bf16),
        *held(returned.reshape(slots, width), slot_weights, base),
    )
    return (layer_out, next_state)


def solution(mesh):
    in_specs = (
        P("ep", "tp"),
        P("ep", None, "tp"),
        P(),
        P(None, "tp"),
        P(None, "tp"),
        P(None, "tp"),
        P("tp", None),
        P(None, "tp"),
        P("tp"),
        P("tp", None),
        P(None, "tp"),
        P("tp"),
        P("tp"),
        P("tp"),
        P("tp"),
        P(None, "tp"),
        P(),
        P("ep", None),
        P("ep", None),
        P("ep", None, "tp"),
        P("ep", None, "tp"),
        P("ep", "tp", None),
        P(None, "tp"),
        P(None, "tp"),
        P("tp", None),
        P(),
    )
    out_specs = (P("ep", "tp"), P("ep", None, "tp"))
    return jax.shard_map(local, mesh=mesh, in_specs=in_specs, out_specs=out_specs, check_vma=False)
```

```python
import jax
import jax.numpy as jnp
from jax import lax
from jax.experimental import pallas as pl
from jax.experimental.pallas import tpu as pltpu
from jax.sharding import PartitionSpec as P


HEAD = 64
f32 = jnp.float32
bf16 = jnp.bfloat16

FIRST = {"tp": 10, "ep": 17}

norm_eps = 1e-06
head_eps = 0.00064
key_eps = 1e-06


def dot(a, b):
    return jnp.dot(a, b, preferred_element_type=f32)


def split_dot(a, b):
    high = a.astype(bf16)
    low = (a - high.astype(f32)).astype(bf16)
    return dot(high, b) + dot(low, b)


def call(kernel, outs, *args, **kwargs):
    params = pltpu.CompilerParams(vmem_limit_bytes=12 << 20)
    return pl.pallas_call(
        kernel, out_shape=outs, compiler_params=params, **kwargs
    )(*args)


def shape(dims, dtype):
    return jax.ShapeDtypeStruct(dims, dtype)


def head_sum(x):
    first = lax.broadcasted_iota(jnp.int32, x.shape, 1) < HEAD
    left = jnp.sum(jnp.where(first, x, 0.0), axis=1, keepdims=True)
    right = jnp.sum(jnp.where(first, 0.0, x), axis=1, keepdims=True)
    return jnp.where(first, left, right)


def same_head():
    rows = lax.broadcasted_iota(jnp.int32, (2 * HEAD, 2 * HEAD), 0) // HEAD
    cols = lax.broadcasted_iota(jnp.int32, (2 * HEAD, 2 * HEAD), 1) // HEAD
    return jnp.where(rows == cols, 1.0, 0.0).astype(bf16)


def own_channel():
    rows = lax.broadcasted_iota(jnp.int32, (HEAD, 2 * HEAD), 0)
    cols = lax.broadcasted_iota(jnp.int32, (HEAD, 2 * HEAD), 1) % HEAD
    return rows == cols


def dot_t(a, b):
    return lax.dot_general(a, b, (((1,), (1,)), ((), ())), preferred_element_type=f32)


def message_kernel(place, tokens, gain, decay_down, iclr_down, out):
    rows = lax.broadcasted_iota(jnp.int32, gain.shape, 0)
    own = jnp.sum(jnp.where(rows == place[0], gain[...].astype(f32), 0.0), axis=0, keepdims=True)
    scaled = (tokens[...].astype(f32) * own).astype(bf16)
    count, seqs, width = out.shape
    rank = decay_down.shape[0]
    pad = jnp.zeros((seqs, width // 3 - rank), f32)
    whole = jnp.concatenate(
        [
            tokens[...].astype(f32),
            dot_t(scaled, decay_down[...]),
            pad,
            dot_t(scaled, iclr_down[...]),
            pad,
        ],
        axis=1,
    ).astype(bf16)
    for p in range(count):
        out[p] = whole


def slot_table(routes, slots, stride):
    top, seqs = routes.shape
    index = lax.broadcasted_iota(jnp.int32, (slots, seqs), 0)
    expert = (index // stride + FIRST["ep"]) % (slots // stride)
    matches = [jnp.where(routes[k : k + 1, :] == expert, 1.0, 0.0) for k in range(top)]
    chosen = matches[0]
    for match in matches[1:]:
        chosen = chosen + match
    earlier = lax.broadcasted_iota(jnp.int32, (seqs, seqs), 0) < lax.broadcasted_iota(
        jnp.int32, (seqs, seqs), 1
    )
    before = dot(chosen.astype(bf16), jnp.where(earlier, 1.0, 0.0).astype(bf16))
    return matches, chosen, before - (index % stride).astype(f32)


def in_three(x):
    high = x.astype(bf16).astype(f32)
    middle = (x - high).astype(bf16).astype(f32)
    return high, middle, x - high - middle


def prep_kernel(
    w_recept,
    w_key,
    w_value,
    decay_up,
    iclr_up,
    state,
    routes,
    route_weights,
    gain,
    decay_base,
    iclr_base,
    key_scale,
    key_mix,
    head_gain,
    weights_out,
    ups_out,
    state_out,
    hit_out,
    notes_out,
    gain_out,
    rows_out,
    sems,
):
    moves = [(w, weights_out.at[i]) for i, w in enumerate((w_recept, w_key, w_value))]
    moves += [(decay_up, ups_out.at[0]), (iclr_up, ups_out.at[1]), (state, state_out)]
    copies = [pltpu.make_async_copy(a, b, sems.at[i]) for i, (a, b) in enumerate(moves)]
    for copy in copies:
        copy.start()
    matches, chosen, offset = slot_table(routes, hit_out.shape[0], 8)
    hit_out[...] = jnp.where(offset == 0.0, chosen, 0.0).astype(bf16)
    noted = offset == -4.0
    weighted = matches[0] * route_weights[0:1, :]
    for k in range(1, len(matches)):
        weighted = weighted + matches[k] * route_weights[k : k + 1, :]
    weight = jnp.sum(jnp.where(noted, weighted, 0.0), axis=1, keepdims=True)
    main = jnp.sum(jnp.where(noted, matches[0], 0.0), axis=1, keepdims=True)
    lanes = lax.broadcasted_iota(jnp.int32, notes_out.shape, 1)
    notes = jnp.zeros(notes_out.shape, f32)
    for i, column in enumerate((*in_three(weight), main)):
        notes = jnp.where(lanes == i, column, notes)
    notes_out[...] = notes.astype(bf16)
    gain_out[...] = gain[...].astype(f32)
    for i, row in enumerate((decay_base, iclr_base, key_scale, key_mix, head_gain)):
        rows_out[i : i + 1, :] = row[...].astype(f32)
    for copy in copies:
        copy.wait()


def gains_kernel(gain, mix, gain_out, mix_out):
    gain_out[...] = gain[...].astype(f32)
    mix_out[...] = mix[...].astype(f32)


def table_kernel(routes, out):
    _, chosen, offset = slot_table(routes, out.shape[0], 4)
    out[...] = jnp.where(offset == 0.0, chosen, 0.0).astype(bf16)


def mixer_in_kernel(
    arrived, state, gain, weights, ups, rows, heads_out, vectors_out
):
    count, seqs, width = arrived.shape
    piece = width // 3
    rank = ups.shape[1]
    decay_base, iclr_base, key_scale, key_mix, head_gain = (rows[i : i + 1, :] for i in range(5))
    tokens = [x[:, :piece].astype(f32) for x in by_feature(arrived, count)]
    squares = tokens[0] * tokens[0]
    for x in tokens[1:]:
        squares = squares + x * x
    scale = lax.rsqrt(
        jnp.sum(squares, axis=1, keepdims=True) * (1.0 / (count * piece)) + norm_eps
    )
    first = jnp.concatenate(
        [
            (x * scale * gain[p : p + 1, :]).astype(bf16)
            for p, x in enumerate(tokens)
        ],
        axis=1,
    )
    low = arrived[0, :, piece:].astype(f32)
    for p in range(1, count):
        low = low + arrived[p, :, piece:].astype(f32)
    low = low * scale
    decay_act = jnp.tanh(low[:, :rank]).astype(bf16)
    rate_act = low[:, piece : piece + rank].astype(bf16)
    recept = dot(first, weights[0]).astype(bf16).astype(f32)
    key = dot(first, weights[1]).astype(bf16).astype(f32)
    value = dot(first, weights[2]).astype(bf16).astype(f32)
    decay_pre = -(decay_base + dot(decay_act, ups[0]))
    softplus = jnp.maximum(decay_pre, 0.0) + jnp.log1p(jnp.exp(-jnp.abs(decay_pre)))
    decay = jnp.exp(-jnp.exp(-softplus - 0.5))
    rate = jax.nn.sigmoid(iclr_base + dot(rate_act, ups[1]))
    scaled = key * key_scale
    removal = scaled * lax.rsqrt(head_sum(scaled * scaled) + key_eps)
    written = key * (1.0 + (rate - 1.0) * key_mix)
    scaled_removal = removal * rate
    together = same_head()
    own = own_channel()

    def against(weights):
        grid = state[...] * weights[:, None, :]
        spread = split_dot(grid.reshape(seqs * HEAD, piece), together)
        return jnp.sum(jnp.where(own, spread.reshape(seqs, HEAD, piece), 0.0), axis=1)

    recall = against(removal)
    read = (
        against(decay * recept)
        - recall * head_sum(scaled_removal * recept)
        + value * head_sum(written * recept)
    )
    centered = read - head_sum(read) * (1.0 / HEAD)
    variance = head_sum(centered * centered) * (1.0 / HEAD)
    head_out = (centered * lax.rsqrt(variance + head_eps) * head_gain).astype(bf16)
    for p in range(count):
        heads_out[p] = head_out
    for i, v in enumerate((removal, decay, scaled_removal, value, written)):
        vectors_out[i] = v


def state_kernel(state, vectors, out):
    seqs, _, width = state.shape
    removal, decay, scaled_removal, value, written = (
        vectors[i][:, None, :] for i in range(5)
    )
    together = same_head()
    grid = state[...]
    recall = split_dot((grid * removal).reshape(seqs * HEAD, width), together)
    spread = jnp.where(own_channel(), value, 0.0).astype(bf16).reshape(seqs * HEAD, width)
    values = dot(spread, together)
    out[...] = (
        grid * decay
        - recall.reshape(seqs, HEAD, width) * scaled_removal
        + values.reshape(seqs, HEAD, width) * written
    )


def dispatch_kernel(heads, w_out, tokens, hit, notes, residual_out, outgoing):
    count = heads.shape[0]
    rows = jnp.concatenate([x[...] for x in by_feature(heads, count)], axis=1)
    mixed = dot(rows, w_out[...]).astype(bf16).astype(f32)
    residual = (tokens[...].astype(f32) + mixed).astype(bf16)
    residual_out[...] = residual
    outgoing[...] = (dot(hit[...], residual) + notes[...].astype(f32)).astype(bf16)


def spread_kernel(arrived, out, notes_out):
    count, slots, _ = out.shape
    slot = lax.broadcasted_iota(jnp.int32, (slots, 2 * slots), 0)
    place = lax.broadcasted_iota(jnp.int32, (slots, 2 * slots), 1) - (slot // 4 * 8 + slot % 4)
    rows = dot(jnp.where(place == 0, 1.0, 0.0).astype(bf16), arrived[...]).astype(bf16)
    for p in range(count):
        out[p] = rows
    notes_out[...] = dot(jnp.where(place == 4, 1.0, 0.0).astype(bf16), arrived[...])


def expert_kernel(
    arrived, notes, gain, mix, gate, up, down, dense_gate, dense_up, dense_down, out
):
    count, _, piece = arrived.shape
    pieces = [x[...].astype(f32) for x in by_feature(arrived, count)]
    squares = pieces[0] * pieces[0]
    for x in pieces[1:]:
        squares = squares + x * x
    scale = lax.rsqrt(
        jnp.sum(squares, axis=1, keepdims=True) * (1.0 / (count * piece)) + norm_eps
    )
    normed = [
        (x * scale * gain[p : p + 1, :]).astype(bf16) for p, x in enumerate(pieces)
    ]
    mixed = normed[0].astype(f32) * mix[0:1, :]
    for p in range(1, count):
        mixed = mixed + normed[p].astype(f32) * mix[p : p + 1, :]
    mix_gate = jax.nn.sigmoid(jnp.sum(mixed, axis=1, keepdims=True))
    weight = notes[:, 0:1] + notes[:, 1:2] + notes[:, 2:3]
    dense_weight = mix_gate * notes[:, 3:4]
    second = jnp.concatenate(normed, axis=1)
    hidden = (jax.nn.silu(dot(second, gate[...])) * dot(second, up[...])).astype(bf16)
    dense_hidden = (
        jax.nn.silu(dot_t(second, dense_gate[...])) * dot_t(second, dense_up[...])
    ).astype(bf16)
    for p, t in enumerate(member_order(count, "tp")):
        cols = slice(t * piece, (t + 1) * piece)
        out[p] = (
            weight * dot(hidden, down[:, cols])
            + dense_weight * dot(dense_hidden, dense_down[:, cols])
        ).astype(bf16)


def total_kernel(partial, out):
    total = partial[0].astype(f32)
    for p in range(1, partial.shape[0]):
        total = total + partial[p].astype(f32)
    out[...] = total.astype(bf16)


def base_kernel(residual, out):
    out[...] = residual[...].astype(f32)


def final_kernel(returned, table, base, out):
    routed = lax.dot_general(
        table[...], returned[...], (((0,), (0,)), ((), ())), preferred_element_type=f32
    )
    out[...] = (base[...] + routed).astype(bf16)


def member_order(count, axis):
    return [(i + FIRST[axis]) % count for i in range(count)]


def by_feature(ref, count):
    return [ref.at[(t - FIRST["tp"]) % count] for t in range(count)]


def exchange(value, axis):
    order = member_order(lax.axis_size(axis), axis)
    return lax.all_to_all(value, axis, 0, 0, tiled=True, axis_index_groups=[order])


def near(dims, dtype):
    return pltpu.VMEM(dims, dtype)


def far(*values):
    return [pltpu.with_memory_space_constraint(v, pltpu.HBM) for v in values]


def held(*values):
    return [pltpu.with_memory_space_constraint(v, pltpu.VMEM) for v in values]


def local(
    token_rows,
    prior_state,
    first_gain,
    w_recept,
    w_key,
    w_value,
    decay_down,
    decay_up,
    decay_base,
    iclr_down,
    iclr_up,
    iclr_base,
    key_scale,
    key_mix,
    head_gain,
    w_out,
    second_gain,
    routes,
    route_weights,
    exp_gate,
    exp_up,
    exp_down,
    dense_gate,
    dense_up,
    dense_down,
    dense_mix,
):
    seqs, width = token_rows.shape
    count = lax.axis_size("tp")
    groups = lax.axis_size("ep")
    slots = groups * 4
    place = lax.axis_index("tp").reshape(1).astype(jnp.int32)
    row = lambda v: v.reshape(1, width)
    pieces = lambda v: v.reshape(count, width)
    in_smem = pl.BlockSpec(memory_space=pltpu.SMEM)
    in_vmem = pl.BlockSpec(memory_space=pltpu.VMEM)
    message = call(
        message_kernel,
        shape((count, seqs, 3 * width), bf16),
        place,
        *far(token_rows, pieces(first_gain), decay_down.T, iclr_down.T),
        in_specs=[in_smem] + [in_vmem] * 4,
    )
    arrived = exchange(message, "tp")
    weights, ups, state, hit, notes, gain, rows_of = call(
        prep_kernel,
        (
            near((3, *w_key.shape), bf16),
            near((2, *decay_up.shape), bf16),
            near(prior_state.shape, f32),
            near((2 * slots, seqs), bf16),
            near((2 * slots, width), bf16),
            near((count, width), f32),
            near((8, width), f32),
        ),
        *far(
            w_recept,
            w_key,
            w_value,
            decay_up,
            iclr_up,
            prior_state,
            routes.T,
            route_weights.T,
            pieces(first_gain),
            row(decay_base),
            row(iclr_base),
            row(key_scale),
            row(key_mix),
            row(head_gain),
        ),
        in_specs=[pl.BlockSpec(memory_space=pl.ANY)] * 6 + [in_vmem] * 8,
        scratch_shapes=[pltpu.SemaphoreType.DMA((6,))],
    )
    heads, vectors = call(
        mixer_in_kernel,
        (near((count, seqs, width), bf16), near((5, seqs, width), f32)),
        *held(arrived, state, gain, weights, ups, rows_of),
    )
    heads_all = exchange(heads, "tp")
    block = 8
    next_state = call(
        state_kernel,
        shape(prior_state.shape, f32),
        *far(prior_state),
        *held(vectors),
        grid=(seqs // block,),
        in_specs=[
            pl.BlockSpec((block, HEAD, width), lambda i: (i, 0, 0)),
            pl.BlockSpec((5, block, width), lambda i: (0, i, 0)),
        ],
        out_specs=pl.BlockSpec((block, HEAD, width), lambda i: (i, 0, 0)),
    )
    residual, outgoing = call(
        dispatch_kernel,
        (near((seqs, width), bf16), shape((2 * slots, width), bf16)),
        *held(heads_all, w_out, token_rows, hit, notes),
    )
    sent = exchange(outgoing.reshape(groups, 8, width), "ep")
    second_scale, mix_scale = call(
        gains_kernel,
        (near((count, width), f32), near((count, width), f32)),
        *far(pieces(second_gain), pieces(dense_mix)),
    )
    rows, slot_notes = call(
        spread_kernel,
        (shape((count, slots, width), bf16), near((slots, width), f32)),
        *held(sent.reshape(2 * slots, width)),
    )
    gathered = exchange(rows, "tp")
    table = call(table_kernel, near((slots, seqs), bf16), *far(routes.T))
    partial = call(
        expert_kernel,
        shape((count, slots, width), bf16),
        *held(
            gathered,
            slot_notes,
            second_scale,
            mix_scale,
            exp_gate[0],
            exp_up[0],
            exp_down[0],
            dense_gate.T,
            dense_up.T,
            dense_down,
        ),
    )
    expert_out = call(
        total_kernel, shape((slots, width), bf16), *held(exchange(partial, "tp"))
    )
    returned = exchange(expert_out.reshape(groups, 4, width), "ep")
    base = call(base_kernel, near((seqs, width), f32), *held(residual))
    layer_out = call(
        final_kernel,
        shape((seqs, width), bf16),
        *held(returned.reshape(slots, width), table, base),
    )
    return (layer_out, next_state)


def solution(mesh):
    in_specs = (
        P("ep", "tp"),
        P("ep", None, "tp"),
        P(),
        P(None, "tp"),
        P(None, "tp"),
        P(None, "tp"),
        P("tp", None),
        P(None, "tp"),
        P("tp"),
        P("tp", None),
        P(None, "tp"),
        P("tp"),
        P("tp"),
        P("tp"),
        P("tp"),
        P(None, "tp"),
        P(),
        P("ep", None),
        P("ep", None),
        P("ep", None, "tp"),
        P("ep", None, "tp"),
        P("ep", "tp", None),
        P(None, "tp"),
        P(None, "tp"),
        P("tp", None),
        P(),
    )
    out_specs = (P("ep", "tp"), P("ep", None, "tp"))
    return jax.shard_map(local, mesh=mesh, in_specs=in_specs, out_specs=out_specs, check_vma=False)
```

```python
import jax
import jax.numpy as jnp
from jax import lax
from jax.experimental import pallas as pl
from jax.experimental.pallas import tpu as pltpu
from jax.sharding import PartitionSpec as P


HEAD = 64
f32 = jnp.float32
bf16 = jnp.bfloat16

FIRST = {"tokens": 10, "heads": 10, "spread_out": 10, "sums": 10, "send": 21, "back": 21}

PIECE = 6

norm_eps = 1e-06
head_eps = 0.00064
key_eps = 1e-06


def dot(a, b):
    return jnp.dot(a, b, preferred_element_type=f32)


def split_dot(a, b):
    high = a.astype(bf16)
    low = (a - high.astype(f32)).astype(bf16)
    return dot(high, b) + dot(low, b)


def call(kernel, outs, *args, **kwargs):
    params = pltpu.CompilerParams(vmem_limit_bytes=12 << 20)
    return pl.pallas_call(
        kernel, out_shape=outs, compiler_params=params, **kwargs
    )(*args)


def shape(dims, dtype):
    return jax.ShapeDtypeStruct(dims, dtype)


def head_sum(x):
    first = lax.broadcasted_iota(jnp.int32, x.shape, 1) < HEAD
    left = jnp.sum(jnp.where(first, x, 0.0), axis=1, keepdims=True)
    right = jnp.sum(jnp.where(first, 0.0, x), axis=1, keepdims=True)
    return jnp.where(first, left, right)


def same_head():
    rows = lax.broadcasted_iota(jnp.int32, (2 * HEAD, 2 * HEAD), 0) // HEAD
    cols = lax.broadcasted_iota(jnp.int32, (2 * HEAD, 2 * HEAD), 1) // HEAD
    return jnp.where(rows == cols, 1.0, 0.0).astype(bf16)


def own_channel():
    rows = lax.broadcasted_iota(jnp.int32, (HEAD, 2 * HEAD), 0)
    cols = lax.broadcasted_iota(jnp.int32, (HEAD, 2 * HEAD), 1) % HEAD
    return rows == cols


def dot_t(a, b):
    return lax.dot_general(a, b, (((1,), (1,)), ((), ())), preferred_element_type=f32)


def message_kernel(place, tokens, gain, decay_down, iclr_down, out):
    rows = lax.broadcasted_iota(jnp.int32, gain.shape, 0)
    own = jnp.sum(jnp.where(rows == place[0], gain[...].astype(f32), 0.0), axis=0, keepdims=True)
    scaled = (tokens[...].astype(f32) * own).astype(bf16)
    count, seqs, width = out.shape
    rank = decay_down.shape[0]
    pad = jnp.zeros((seqs, width // 3 - rank), f32)
    whole = jnp.concatenate(
        [
            tokens[...].astype(f32),
            dot_t(scaled, decay_down[...]),
            pad,
            dot_t(scaled, iclr_down[...]),
            pad,
        ],
        axis=1,
    ).astype(bf16)
    for p in range(count):
        out[p] = whole


def slot_table(routes, slots, stride, first):
    top, seqs = routes.shape
    index = lax.broadcasted_iota(jnp.int32, (slots, seqs), 0)
    expert = (index // stride + first) % (slots // stride)
    matches = [jnp.where(routes[k : k + 1, :] == expert, 1.0, 0.0) for k in range(top)]
    chosen = matches[0]
    for match in matches[1:]:
        chosen = chosen + match
    earlier = lax.broadcasted_iota(jnp.int32, (seqs, seqs), 0) < lax.broadcasted_iota(
        jnp.int32, (seqs, seqs), 1
    )
    before = dot(chosen.astype(bf16), jnp.where(earlier, 1.0, 0.0).astype(bf16))
    return matches, chosen, before - (index % stride).astype(f32)


def in_three(x):
    high = x.astype(bf16).astype(f32)
    middle = (x - high).astype(bf16).astype(f32)
    return high, middle, x - high - middle


def prep_kernel(
    w_recept,
    w_key,
    w_value,
    decay_up,
    iclr_up,
    state,
    routes,
    route_weights,
    gain,
    decay_base,
    iclr_base,
    key_scale,
    key_mix,
    head_gain,
    weights_out,
    ups_out,
    state_out,
    hit_out,
    notes_out,
    gain_out,
    rows_out,
    sems,
):
    moves = [(w, weights_out.at[i]) for i, w in enumerate((w_recept, w_key, w_value))]
    moves += [(decay_up, ups_out.at[0]), (iclr_up, ups_out.at[1]), (state, state_out)]
    copies = [pltpu.make_async_copy(a, b, sems.at[i]) for i, (a, b) in enumerate(moves)]
    for copy in copies:
        copy.start()
    matches, chosen, offset = slot_table(routes, hit_out.shape[0], PIECE, FIRST["send"])
    hit_out[...] = jnp.where(offset == 0.0, chosen, 0.0).astype(bf16)
    weighted = matches[0] * route_weights[0:1, :]
    for k in range(1, len(matches)):
        weighted = weighted + matches[k] * route_weights[k : k + 1, :]
    lanes = lax.broadcasted_iota(jnp.int32, notes_out.shape, 1)
    notes = jnp.zeros(notes_out.shape, f32)
    for c in range(4):
        noted = offset == c - 4.0
        weight = jnp.sum(jnp.where(noted, weighted, 0.0), axis=1, keepdims=True)
        main = jnp.sum(jnp.where(noted, matches[0], 0.0), axis=1, keepdims=True)
        for i, column in enumerate((*in_three(weight), main)):
            notes = jnp.where(lanes == 4 * c + i, column, notes)
    rows = lax.broadcasted_iota(jnp.int32, notes_out.shape, 0)
    notes_out[...] = jnp.where(rows % PIECE == 4, notes, 0.0).astype(bf16)
    gain_out[...] = gain[...].astype(f32)
    for i, row in enumerate((decay_base, iclr_base, key_scale, key_mix, head_gain)):
        rows_out[i : i + 1, :] = row[...].astype(f32)
    for copy in copies:
        copy.wait()


def gains_kernel(gain, mix, gain_out, mix_out):
    gain_out[...] = gain[...].astype(f32)
    mix_out[...] = mix[...].astype(f32)


def table_kernel(routes, out):
    _, chosen, offset = slot_table(routes, out.shape[0], 4, FIRST["back"])
    out[...] = jnp.where(offset == 0.0, chosen, 0.0).astype(bf16)


def mixer_in_kernel(
    arrived, state, gain, weights, ups, rows, heads_out, vectors_out
):
    count, seqs, width = arrived.shape
    piece = width // 3
    rank = ups.shape[1]
    decay_base, iclr_base, key_scale, key_mix, head_gain = (rows[i : i + 1, :] for i in range(5))
    tokens = [x[:, :piece].astype(f32) for x in by_feature(arrived, count, "tokens")]
    squares = tokens[0] * tokens[0]
    for x in tokens[1:]:
        squares = squares + x * x
    scale = lax.rsqrt(
        jnp.sum(squares, axis=1, keepdims=True) * (1.0 / (count * piece)) + norm_eps
    )
    first = jnp.concatenate(
        [
            (x * scale * gain[p : p + 1, :]).astype(bf16)
            for p, x in enumerate(tokens)
        ],
        axis=1,
    )
    low = arrived[0, :, piece:].astype(f32)
    for p in range(1, count):
        low = low + arrived[p, :, piece:].astype(f32)
    low = low * scale
    decay_act = jnp.tanh(low[:, :rank]).astype(bf16)
    rate_act = low[:, piece : piece + rank].astype(bf16)
    projected = dot(first, jnp.concatenate([weights[i] for i in range(3)], axis=1))
    projected = projected.astype(bf16).astype(f32)
    recept, key, value = (projected[:, i * piece : (i + 1) * piece] for i in range(3))
    decay_pre = -(decay_base + dot(decay_act, ups[0]))
    softplus = jnp.maximum(decay_pre, 0.0) + jnp.log1p(jnp.exp(-jnp.abs(decay_pre)))
    decay = jnp.exp(-jnp.exp(-softplus - 0.5))
    rate = jax.nn.sigmoid(iclr_base + dot(rate_act, ups[1]))
    scaled = key * key_scale
    removal = scaled * lax.rsqrt(head_sum(scaled * scaled) + key_eps)
    written = key * (1.0 + (rate - 1.0) * key_mix)
    scaled_removal = removal * rate
    together = same_head()
    own = own_channel()

    def against(weights):
        grid = state[...] * weights[:, None, :]
        spread = split_dot(grid.reshape(seqs * HEAD, piece), together)
        return jnp.sum(jnp.where(own, spread.reshape(seqs, HEAD, piece), 0.0), axis=1)

    recall = against(removal)
    read = (
        against(decay * recept)
        - recall * head_sum(scaled_removal * recept)
        + value * head_sum(written * recept)
    )
    centered = read - head_sum(read) * (1.0 / HEAD)
    variance = head_sum(centered * centered) * (1.0 / HEAD)
    head_out = (centered * lax.rsqrt(variance + head_eps) * head_gain).astype(bf16)
    for p in range(count):
        heads_out[p] = head_out
    for i, v in enumerate((removal, decay, scaled_removal, value, written)):
        vectors_out[i] = v


def state_kernel(state, vectors, out):
    seqs, _, width = state.shape
    removal, decay, scaled_removal, value, written = (
        vectors[i][:, None, :] for i in range(5)
    )
    together = same_head()
    grid = state[...]
    recall = split_dot((grid * removal).reshape(seqs * HEAD, width), together)
    spread = jnp.where(own_channel(), value, 0.0).astype(bf16).reshape(seqs * HEAD, width)
    values = dot(spread, together)
    out[...] = (
        grid * decay
        - recall.reshape(seqs, HEAD, width) * scaled_removal
        + values.reshape(seqs, HEAD, width) * written
    )


def dispatch_kernel(heads, w_out, tokens, hit, notes, residual_out, outgoing):
    count = heads.shape[0]
    rows = jnp.concatenate([x[...] for x in by_feature(heads, count, "heads")], axis=1)
    mixed = dot(rows, w_out[...]).astype(bf16).astype(f32)
    residual = (tokens[...].astype(f32) + mixed).astype(bf16)
    residual_out[...] = residual
    outgoing[...] = (dot(hit[...], residual) + notes[...].astype(f32)).astype(bf16)


def spread_kernel(arrived, out, notes_out):
    count, slots, width = out.shape
    size = arrived.shape[0]
    slot = lax.broadcasted_iota(jnp.int32, (slots, size), 0)
    place = lax.broadcasted_iota(jnp.int32, (slots, size), 1) - slot // 4 * PIECE
    rows = dot(jnp.where(place == slot % 4, 1.0, 0.0).astype(bf16), arrived[...]).astype(bf16)
    for p in range(count):
        out[p] = rows
    notes = dot(jnp.where(place == 4, 1.0, 0.0).astype(bf16), arrived[...])
    lane = lax.broadcasted_iota(jnp.int32, (slots, width), 1)
    own = lax.broadcasted_iota(jnp.int32, (slots, width), 0) % 4
    notes_out[...] = jnp.where(lane // 4 == own, notes, 0.0)


def expert_kernel(
    arrived, notes, gain, mix, gate, up, down, dense_gate, dense_up, dense_down, out
):
    count, _, piece = arrived.shape
    pieces = [x[...].astype(f32) for x in by_feature(arrived, count, "spread_out")]
    squares = pieces[0] * pieces[0]
    for x in pieces[1:]:
        squares = squares + x * x
    scale = lax.rsqrt(
        jnp.sum(squares, axis=1, keepdims=True) * (1.0 / (count * piece)) + norm_eps
    )
    normed = [
        (x * scale * gain[p : p + 1, :]).astype(bf16) for p, x in enumerate(pieces)
    ]
    mixed = normed[0].astype(f32) * mix[0:1, :]
    for p in range(1, count):
        mixed = mixed + normed[p].astype(f32) * mix[p : p + 1, :]
    mix_gate = jax.nn.sigmoid(jnp.sum(mixed, axis=1, keepdims=True))
    flagged = lax.broadcasted_iota(jnp.int32, notes.shape, 1) % 4 == 3
    weight = jnp.sum(jnp.where(flagged, 0.0, notes[...]), axis=1, keepdims=True)
    main = jnp.sum(jnp.where(flagged, notes[...], 0.0), axis=1, keepdims=True)
    second = jnp.concatenate(normed, axis=1)
    units = gate.shape[1]
    both = dot(second, jnp.concatenate([gate[...], up[...]], axis=1))
    hidden = jax.nn.silu(both[:, :units]) * both[:, units:] * weight
    small = dense_gate.shape[0]
    dense = dot_t(second, jnp.concatenate([dense_gate[...], dense_up[...]], axis=0))
    dense_hidden = jax.nn.silu(dense[:, :small]) * dense[:, small:] * (mix_gate * main)
    joined = jnp.concatenate([hidden, dense_hidden], axis=1).astype(bf16)
    order = member_order(count, "sums")
    for t in range(0, count, 2):
        cols = slice(t * piece, (t + 2) * piece)
        block = dot(joined, jnp.concatenate([down[:, cols], dense_down[:, cols]], axis=0))
        for i in range(2):
            out[order.index(t + i)] = block[:, i * piece : (i + 1) * piece].astype(bf16)


def total_kernel(partial, out):
    total = partial[0].astype(f32)
    for p in range(1, partial.shape[0]):
        total = total + partial[p].astype(f32)
    turn = (FIRST["back"] - FIRST["send"]) * 4 % out.shape[0]
    if turn:
        total = jnp.concatenate([total[turn:], total[:turn]], axis=0)
    out[...] = total.astype(bf16)


def base_kernel(residual, out):
    out[...] = residual[...].astype(f32)


def final_kernel(returned, table, base, out):
    routed = lax.dot_general(
        table[...], returned[...], (((0,), (0,)), ((), ())), preferred_element_type=f32
    )
    out[...] = (base[...] + routed).astype(bf16)


def member_order(count, name):
    return [(i + FIRST[name]) % count for i in range(count)]


def by_feature(ref, count, name):
    return [ref.at[(t - FIRST[name]) % count] for t in range(count)]


def exchange(value, axis, name):
    order = member_order(lax.axis_size(axis), name)
    return lax.all_to_all(value, axis, 0, 0, tiled=True, axis_index_groups=[order])


def near(dims, dtype):
    return pltpu.VMEM(dims, dtype)


def far(*values):
    return [pltpu.with_memory_space_constraint(v, pltpu.HBM) for v in values]


def held(*values):
    return [pltpu.with_memory_space_constraint(v, pltpu.VMEM) for v in values]


def local(
    token_rows,
    prior_state,
    first_gain,
    w_recept,
    w_key,
    w_value,
    decay_down,
    decay_up,
    decay_base,
    iclr_down,
    iclr_up,
    iclr_base,
    key_scale,
    key_mix,
    head_gain,
    w_out,
    second_gain,
    routes,
    route_weights,
    exp_gate,
    exp_up,
    exp_down,
    dense_gate,
    dense_up,
    dense_down,
    dense_mix,
):
    seqs, width = token_rows.shape
    count = lax.axis_size("tp")
    groups = lax.axis_size("ep")
    slots = groups * 4
    sent_rows = groups * PIECE
    place = lax.axis_index("tp").reshape(1).astype(jnp.int32)
    row = lambda v: v.reshape(1, width)
    pieces = lambda v: v.reshape(count, width)
    in_smem = pl.BlockSpec(memory_space=pltpu.SMEM)
    in_vmem = pl.BlockSpec(memory_space=pltpu.VMEM)
    message = call(
        message_kernel,
        shape((count, seqs, 3 * width), bf16),
        place,
        *far(token_rows, pieces(first_gain), decay_down.T, iclr_down.T),
        in_specs=[in_smem] + [in_vmem] * 4,
    )
    arrived = exchange(message, "tp", "tokens")
    weights, ups, state, hit, notes, gain, rows_of = call(
        prep_kernel,
        (
            near((3, *w_key.shape), bf16),
            near((2, *decay_up.shape), bf16),
            near(prior_state.shape, f32),
            near((sent_rows, seqs), bf16),
            near((sent_rows, width), bf16),
            near((count, width), f32),
            near((8, width), f32),
        ),
        *far(
            w_recept,
            w_key,
            w_value,
            decay_up,
            iclr_up,
            prior_state,
            routes.T,
            route_weights.T,
            pieces(first_gain),
            row(decay_base),
            row(iclr_base),
            row(key_scale),
            row(key_mix),
            row(head_gain),
        ),
        in_specs=[pl.BlockSpec(memory_space=pl.ANY)] * 6 + [in_vmem] * 8,
        scratch_shapes=[pltpu.SemaphoreType.DMA((6,))],
    )
    heads, vectors = call(
        mixer_in_kernel,
        (near((count, seqs, width), bf16), near((5, seqs, width), f32)),
        *held(arrived, state, gain, weights, ups, rows_of),
    )
    heads_all = exchange(heads, "tp", "heads")
    block = 8
    next_state = call(
        state_kernel,
        shape(prior_state.shape, f32),
        *far(prior_state),
        *held(vectors),
        grid=(seqs // block,),
        in_specs=[
            pl.BlockSpec((block, HEAD, width), lambda i: (i, 0, 0)),
            pl.BlockSpec((5, block, width), lambda i: (0, i, 0)),
        ],
        out_specs=pl.BlockSpec((block, HEAD, width), lambda i: (i, 0, 0)),
    )
    residual, outgoing = call(
        dispatch_kernel,
        (near((seqs, width), bf16), shape((sent_rows, width), bf16)),
        *held(heads_all, w_out, token_rows, hit, notes),
    )
    sent = exchange(outgoing.reshape(groups, PIECE // 2, 2, width), "ep", "send")
    second_scale, mix_scale = call(
        gains_kernel,
        (near((count, width), f32), near((count, width), f32)),
        *far(pieces(second_gain), pieces(dense_mix)),
    )
    rows, slot_notes = call(
        spread_kernel,
        (shape((count, slots, width), bf16), near((slots, width), f32)),
        *held(sent.reshape(sent_rows, width)),
    )
    gathered = exchange(rows, "tp", "spread_out")
    table = call(table_kernel, near((slots, seqs), bf16), *far(routes.T))
    partial = call(
        expert_kernel,
        shape((count, slots, width), bf16),
        *held(
            gathered,
            slot_notes,
            second_scale,
            mix_scale,
            exp_gate[0],
            exp_up[0],
            exp_down[0],
            dense_gate.T,
            dense_up.T,
            dense_down,
        ),
    )
    expert_out = call(
        total_kernel,
        shape((slots, width), bf16),
        *held(exchange(partial, "tp", "sums")),
    )
    returned = exchange(expert_out.reshape(groups, 4, width), "ep", "back")
    base = call(base_kernel, near((seqs, width), f32), *held(residual))
    layer_out = call(
        final_kernel,
        shape((seqs, width), bf16),
        *held(returned.reshape(slots, width), table, base),
    )
    return (layer_out, next_state)


def solution(mesh):
    in_specs = (
        P("ep", "tp"),
        P("ep", None, "tp"),
        P(),
        P(None, "tp"),
        P(None, "tp"),
        P(None, "tp"),
        P("tp", None),
        P(None, "tp"),
        P("tp"),
        P("tp", None),
        P(None, "tp"),
        P("tp"),
        P("tp"),
        P("tp"),
        P("tp"),
        P(None, "tp"),
        P(),
        P("ep", None),
        P("ep", None),
        P("ep", None, "tp"),
        P("ep", None, "tp"),
        P("ep", "tp", None),
        P(None, "tp"),
        P(None, "tp"),
        P("tp", None),
        P(),
    )
    out_specs = (P("ep", "tp"), P("ep", None, "tp"))
    return jax.shard_map(local, mesh=mesh, in_specs=in_specs, out_specs=out_specs, check_vma=False)
```

```python
import jax
import jax.numpy as jnp
from jax import lax
from jax.experimental import pallas as pl
from jax.experimental.pallas import tpu as pltpu
from jax.sharding import PartitionSpec as P


HEAD = 64
f32 = jnp.float32
bf16 = jnp.bfloat16

FIRST = {"tokens": 10, "heads": 10, "spread_out": 10, "sums": 10, "send": 21, "back": 21}

PIECE = 6

norm_eps = 1e-06
head_eps = 0.00064
key_eps = 1e-06


def dot(a, b):
    return jnp.dot(a, b, preferred_element_type=f32)


def split_dot(a, b):
    high = a.astype(bf16)
    low = (a - high.astype(f32)).astype(bf16)
    return dot(high, b) + dot(low, b)


def call(kernel, outs, *args, **kwargs):
    params = pltpu.CompilerParams(vmem_limit_bytes=12 << 20)
    return pl.pallas_call(kernel, out_shape=outs, compiler_params=params, **kwargs)(*args)


def shape(dims, dtype):
    return jax.ShapeDtypeStruct(dims, dtype)


def head_sum(x):
    first = lax.broadcasted_iota(jnp.int32, x.shape, 1) < HEAD
    left = jnp.sum(jnp.where(first, x, 0.0), axis=1, keepdims=True)
    right = jnp.sum(jnp.where(first, 0.0, x), axis=1, keepdims=True)
    return jnp.where(first, left, right)


def same_head():
    rows = lax.broadcasted_iota(jnp.int32, (2 * HEAD, 2 * HEAD), 0) // HEAD
    cols = lax.broadcasted_iota(jnp.int32, (2 * HEAD, 2 * HEAD), 1) // HEAD
    return jnp.where(rows == cols, 1.0, 0.0).astype(bf16)


def own_channel():
    rows = lax.broadcasted_iota(jnp.int32, (HEAD, 2 * HEAD), 0)
    cols = lax.broadcasted_iota(jnp.int32, (HEAD, 2 * HEAD), 1) % HEAD
    return rows == cols


def dot_t(a, b):
    return lax.dot_general(a, b, (((1,), (1,)), ((), ())), preferred_element_type=f32)


def message_kernel(place, tokens, gain, decay_down, iclr_down, out):
    rows = lax.broadcasted_iota(jnp.int32, gain.shape, 0)
    own = jnp.sum(jnp.where(rows == place[0], gain[...].astype(f32), 0.0), axis=0, keepdims=True)
    values = tokens[...].astype(f32)
    scaled = (values * own).astype(bf16)
    width = tokens.shape[1]
    low = dot_t(scaled, jnp.concatenate([decay_down[...], iclr_down[...]], axis=0))
    squares = in_three(jnp.sum(values * values, axis=1, keepdims=True))
    lanes = lax.broadcasted_iota(jnp.int32, (8, width - HEAD), 1)
    corner = jnp.zeros(lanes.shape, f32)
    for g in range(3):
        for i in range(3):
            corner = jnp.where(lanes == 3 * g + i, squares[i][8 * g : 8 * g + 8], corner)
    rest = low[:, width:]
    tail = jnp.concatenate([rest[:16], jnp.concatenate([rest[16:], corner], axis=0)], axis=1)
    whole = jnp.concatenate([scaled.astype(f32), low[:, :width], tail], axis=0).astype(bf16)
    for p in range(out.shape[0]):
        out[p] = whole


def slot_table(routes, slots, stride, first):
    top, seqs = routes.shape
    index = lax.broadcasted_iota(jnp.int32, (slots, seqs), 0)
    expert = (index // stride + first) % (slots // stride)
    matches = [jnp.where(routes[k : k + 1, :] == expert, 1.0, 0.0) for k in range(top)]
    chosen = matches[0]
    for match in matches[1:]:
        chosen = chosen + match
    earlier = lax.broadcasted_iota(jnp.int32, (seqs, seqs), 0) < lax.broadcasted_iota(
        jnp.int32, (seqs, seqs), 1
    )
    before = dot(chosen.astype(bf16), jnp.where(earlier, 1.0, 0.0).astype(bf16))
    return matches, chosen, before - (index % stride).astype(f32)


def in_three(x):
    high = x.astype(bf16).astype(f32)
    middle = (x - high).astype(bf16).astype(f32)
    return high, middle, x - high - middle


def prep_kernel(
    w_recept,
    w_key,
    w_value,
    decay_up,
    iclr_up,
    state,
    routes,
    route_weights,
    decay_base,
    iclr_base,
    key_scale,
    key_mix,
    head_gain,
    weights_out,
    ups_out,
    state_out,
    hit_out,
    notes_out,
    rows_out,
    sems,
):
    moves = [(w, weights_out.at[i]) for i, w in enumerate((w_recept, w_key, w_value))]
    moves += [(decay_up, ups_out.at[0]), (iclr_up, ups_out.at[1]), (state, state_out)]
    copies = [pltpu.make_async_copy(a, b, sems.at[i]) for i, (a, b) in enumerate(moves)]
    for copy in copies:
        copy.start()
    matches, chosen, offset = slot_table(routes, hit_out.shape[0], PIECE, FIRST["send"])
    hit_out[...] = jnp.where(offset == 0.0, chosen, 0.0).astype(bf16)
    weighted = matches[0] * route_weights[0:1, :]
    for k in range(1, len(matches)):
        weighted = weighted + matches[k] * route_weights[k : k + 1, :]
    lanes = lax.broadcasted_iota(jnp.int32, notes_out.shape, 1)
    notes = jnp.zeros(notes_out.shape, f32)
    for c in range(4):
        noted = offset == c - 4.0
        weight = jnp.sum(jnp.where(noted, weighted, 0.0), axis=1, keepdims=True)
        main = jnp.sum(jnp.where(noted, matches[0], 0.0), axis=1, keepdims=True)
        for i, column in enumerate((*in_three(weight), main)):
            notes = jnp.where(lanes == 4 * c + i, column, notes)
    rows = lax.broadcasted_iota(jnp.int32, notes_out.shape, 0)
    notes_out[...] = jnp.where(rows % PIECE == 4, notes, 0.0).astype(bf16)
    for i, row in enumerate((decay_base, iclr_base, key_scale, key_mix, head_gain)):
        rows_out[i : i + 1, :] = row[...].astype(f32)
    for copy in copies:
        copy.wait()


def gains_kernel(gain, mix, gain_out, mix_out):
    gain_out[...] = gain[...].astype(f32)
    mix_out[...] = mix[...].astype(f32)


def table_kernel(routes, out):
    _, chosen, offset = slot_table(routes, out.shape[0], 4, FIRST["back"])
    out[...] = jnp.where(offset == 0.0, chosen, 0.0).astype(bf16)


def mixer_in_kernel(arrived, state, weights, ups, rows, heads_out, vectors_out):
    count, _, piece = arrived.shape
    seqs = state.shape[0]
    rank = ups.shape[1]
    split = piece - rank
    decay_base, iclr_base, key_scale, key_mix, head_gain = (rows[i : i + 1, :] for i in range(5))
    first = jnp.concatenate([x[:seqs] for x in by_feature(arrived, count, "tokens")], axis=1)
    low = arrived[0, seqs:].astype(f32)
    for p in range(1, count):
        low = low + arrived[p, seqs:].astype(f32)
    tail = low[seqs:]
    lanes = lax.broadcasted_iota(jnp.int32, (8, piece), 1) - HEAD
    squares = jnp.concatenate(
        [
            jnp.sum(
                jnp.where((lanes >= 3 * g) & (lanes < 3 * g + 3), tail[8:], 0.0),
                axis=1,
                keepdims=True,
            )
            for g in range(3)
        ],
        axis=0,
    )
    scale = lax.rsqrt(squares * (1.0 / (count * piece)) + norm_eps)
    near_low = low[:seqs] * scale
    far_low = jnp.concatenate([tail[:, :HEAD], tail[:8, HEAD:]], axis=0) * scale
    decay_act = jnp.tanh(near_low[:, :rank]).astype(bf16)
    rate_near = near_low[:, rank:].astype(bf16)
    rate_far = far_low.astype(bf16)
    recept, key, value = (
        (dot(first, weights[i]) * scale).astype(bf16).astype(f32) for i in range(3)
    )
    decay_pre = -(decay_base + dot(decay_act, ups[0]))
    softplus = jnp.maximum(decay_pre, 0.0) + jnp.log1p(jnp.exp(-jnp.abs(decay_pre)))
    decay = jnp.exp(-jnp.exp(-softplus - 0.5))
    rate = jax.nn.sigmoid(iclr_base + dot(rate_near, ups[1, :split]) + dot(rate_far, ups[1, split:]))
    scaled = key * key_scale
    removal = scaled * lax.rsqrt(head_sum(scaled * scaled) + key_eps)
    written = key * (1.0 + (rate - 1.0) * key_mix)
    scaled_removal = removal * rate
    together = same_head()
    own = own_channel()

    def against(weights):
        grid = state[...] * weights[:, None, :]
        spread = split_dot(grid.reshape(seqs * HEAD, piece), together)
        return jnp.sum(jnp.where(own, spread.reshape(seqs, HEAD, piece), 0.0), axis=1)

    recall = against(removal)
    read = (
        against(decay * recept)
        - recall * head_sum(scaled_removal * recept)
        + value * head_sum(written * recept)
    )
    centered = read - head_sum(read) * (1.0 / HEAD)
    variance = head_sum(centered * centered) * (1.0 / HEAD)
    head_out = (centered * lax.rsqrt(variance + head_eps) * head_gain).astype(bf16)
    for p in range(count):
        heads_out[p] = head_out
    for i, v in enumerate((removal, decay, scaled_removal, value, written)):
        vectors_out[i] = v


def state_kernel(state, vectors, out):
    seqs, _, width = state.shape
    removal, decay, scaled_removal, value, written = (
        vectors[i][:, None, :] for i in range(5)
    )
    together = same_head()
    grid = state[...]
    recall = split_dot((grid * removal).reshape(seqs * HEAD, width), together)
    spread = jnp.where(own_channel(), value, 0.0).astype(bf16).reshape(seqs * HEAD, width)
    values = dot(spread, together)
    out[...] = (
        grid * decay
        - recall.reshape(seqs, HEAD, width) * scaled_removal
        + values.reshape(seqs, HEAD, width) * written
    )


def dispatch_kernel(heads, w_out, tokens, hit, notes, residual_out, outgoing):
    count = heads.shape[0]
    rows = jnp.concatenate([x[...] for x in by_feature(heads, count, "heads")], axis=1)
    mixed = dot(rows, w_out[...]).astype(bf16).astype(f32)
    residual = (tokens[...].astype(f32) + mixed).astype(bf16)
    residual_out[...] = residual
    outgoing[...] = (dot(hit[...], residual) + notes[...].astype(f32)).astype(bf16)


def spread_kernel(arrived, out, notes_out):
    count, slots, width = out.shape
    size = arrived.shape[0]
    slot = lax.broadcasted_iota(jnp.int32, (slots, size), 0)
    place = lax.broadcasted_iota(jnp.int32, (slots, size), 1) - slot // 4 * PIECE
    rows = dot(jnp.where(place == slot % 4, 1.0, 0.0).astype(bf16), arrived[...]).astype(bf16)
    for p in range(count):
        out[p] = rows
    notes = dot(jnp.where(place == 4, 1.0, 0.0).astype(bf16), arrived[...])
    lane = lax.broadcasted_iota(jnp.int32, (slots, width), 1)
    own = lax.broadcasted_iota(jnp.int32, (slots, width), 0) % 4
    notes_out[...] = jnp.where(lane // 4 == own, notes, 0.0)


def expert_kernel(
    arrived,
    notes,
    gain,
    mix,
    gate,
    up,
    down,
    dense_gate,
    dense_up,
    dense_down,
    out,
    made,
    sems,
):
    count, _, piece = arrived.shape
    pieces = [x[...].astype(f32) for x in by_feature(arrived, count, "spread_out")]
    squares = pieces[0] * pieces[0]
    for x in pieces[1:]:
        squares = squares + x * x
    scale = lax.rsqrt(
        jnp.sum(squares, axis=1, keepdims=True) * (1.0 / (count * piece)) + norm_eps
    )
    normed = [
        (x * scale * gain[p : p + 1, :]).astype(bf16) for p, x in enumerate(pieces)
    ]
    mixed = normed[0].astype(f32) * mix[0:1, :]
    for p in range(1, count):
        mixed = mixed + normed[p].astype(f32) * mix[p : p + 1, :]
    mix_gate = jax.nn.sigmoid(jnp.sum(mixed, axis=1, keepdims=True))
    flagged = lax.broadcasted_iota(jnp.int32, notes.shape, 1) % 4 == 3
    weight = jnp.sum(jnp.where(flagged, 0.0, notes[...]), axis=1, keepdims=True)
    main = jnp.sum(jnp.where(flagged, notes[...], 0.0), axis=1, keepdims=True)
    second = jnp.concatenate(normed, axis=1)
    units = gate.shape[1]
    both = dot(second, jnp.concatenate([gate[...], up[...]], axis=1))
    hidden = jax.nn.silu(both[:, :units]) * both[:, units:] * weight
    small = dense_gate.shape[0]
    dense = dot_t(second, jnp.concatenate([dense_gate[...], dense_up[...]], axis=0))
    dense_hidden = jax.nn.silu(dense[:, :small]) * dense[:, small:] * (mix_gate * main)
    joined = jnp.concatenate([hidden, dense_hidden], axis=1).astype(bf16)
    order = member_order(count, "sums")
    copies = []
    for p in range(0, count, 2):
        cols = slice(order[p] * piece, (order[p] + 2) * piece)
        block = dot(joined, jnp.concatenate([down[:, cols], dense_down[:, cols]], axis=0))
        for i in range(2):
            made[p + i] = block[:, i * piece : (i + 1) * piece].astype(bf16)
        if p % 8 == 6:
            part = pl.ds(p - 6, 8)
            copies.append(pltpu.make_async_copy(made.at[part], out.at[part], sems.at[p // 8]))
            copies[-1].start()
    for copy in copies:
        copy.wait()


def total_kernel(partial, out):
    total = partial[0].astype(f32)
    for p in range(1, partial.shape[0]):
        total = total + partial[p].astype(f32)
    turn = (FIRST["back"] - FIRST["send"]) * 4 % out.shape[0]
    if turn:
        total = jnp.concatenate([total[turn:], total[:turn]], axis=0)
    out[...] = total.astype(bf16)


def base_kernel(residual, out):
    out[...] = residual[...].astype(f32)


def final_kernel(returned, table, base, out):
    routed = lax.dot_general(
        table[...], returned[...], (((0,), (0,)), ((), ())), preferred_element_type=f32
    )
    out[...] = (base[...] + routed).astype(bf16)


def member_order(count, name):
    return [(i + FIRST[name]) % count for i in range(count)]


def by_feature(ref, count, name):
    return [ref.at[(t - FIRST[name]) % count] for t in range(count)]


def exchange(value, axis, name):
    order = member_order(lax.axis_size(axis), name)
    return lax.all_to_all(value, axis, 0, 0, tiled=True, axis_index_groups=[order])


def near(dims, dtype):
    return pltpu.VMEM(dims, dtype)


def far(*values):
    return [pltpu.with_memory_space_constraint(v, pltpu.HBM) for v in values]


def held(*values):
    return [pltpu.with_memory_space_constraint(v, pltpu.VMEM) for v in values]


def local(
    token_rows,
    prior_state,
    first_gain,
    w_recept,
    w_key,
    w_value,
    decay_down,
    decay_up,
    decay_base,
    iclr_down,
    iclr_up,
    iclr_base,
    key_scale,
    key_mix,
    head_gain,
    w_out,
    second_gain,
    routes,
    route_weights,
    exp_gate,
    exp_up,
    exp_down,
    dense_gate,
    dense_up,
    dense_down,
    dense_mix,
):
    seqs, width = token_rows.shape
    count = lax.axis_size("tp")
    groups = lax.axis_size("ep")
    slots = groups * 4
    sent_rows = groups * PIECE
    place = lax.axis_index("tp").reshape(1).astype(jnp.int32)
    row = lambda v: v.reshape(1, width)
    pieces = lambda v: v.reshape(count, width)
    in_smem = pl.BlockSpec(memory_space=pltpu.SMEM)
    in_vmem = pl.BlockSpec(memory_space=pltpu.VMEM)
    message = call(
        message_kernel,
        shape((count, 2 * seqs + 16, width), bf16),
        place,
        *far(token_rows, pieces(first_gain), decay_down.T, iclr_down.T),
        in_specs=[in_smem] + [in_vmem] * 4,
    )
    arrived = exchange(message, "tp", "tokens")
    weights, ups, state, hit, notes, rows_of = call(
        prep_kernel,
        (
            near((3, *w_key.shape), bf16),
            near((2, *decay_up.shape), bf16),
            near(prior_state.shape, f32),
            near((sent_rows, seqs), bf16),
            near((sent_rows, width), bf16),
            near((8, width), f32),
        ),
        *far(
            w_recept,
            w_key,
            w_value,
            decay_up,
            iclr_up,
            prior_state,
            routes.T,
            route_weights.T,
            row(decay_base),
            row(iclr_base),
            row(key_scale),
            row(key_mix),
            row(head_gain),
        ),
        in_specs=[pl.BlockSpec(memory_space=pl.ANY)] * 6 + [in_vmem] * 7,
        scratch_shapes=[pltpu.SemaphoreType.DMA((6,))],
    )
    heads, vectors = call(
        mixer_in_kernel,
        (near((count, seqs, width), bf16), near((5, seqs, width), f32)),
        *held(arrived, state, weights, ups, rows_of),
    )
    heads_all = exchange(heads, "tp", "heads")
    block = 8
    next_state = call(
        state_kernel,
        shape(prior_state.shape, f32),
        *far(prior_state),
        *held(vectors),
        grid=(seqs // block,),
        in_specs=[
            pl.BlockSpec((block, HEAD, width), lambda i: (i, 0, 0)),
            pl.BlockSpec((5, block, width), lambda i: (0, i, 0)),
        ],
        out_specs=pl.BlockSpec((block, HEAD, width), lambda i: (i, 0, 0)),
    )
    residual, outgoing = call(
        dispatch_kernel,
        (near((seqs, width), bf16), shape((sent_rows, width), bf16)),
        *held(heads_all, w_out, token_rows, hit, notes),
    )
    sent = exchange(outgoing.reshape(groups, PIECE // 2, 2, width), "ep", "send")
    second_scale, mix_scale = call(
        gains_kernel,
        (near((count, width), f32), near((count, width), f32)),
        *far(pieces(second_gain), pieces(dense_mix)),
    )
    rows, slot_notes = call(
        spread_kernel,
        (shape((count, slots, width), bf16), near((slots, width), f32)),
        *held(sent.reshape(sent_rows, width)),
    )
    gathered = exchange(rows, "tp", "spread_out")
    table = call(table_kernel, near((slots, seqs), bf16), *far(routes.T))
    partial = call(
        expert_kernel,
        shape((count, slots, width), bf16),
        *held(
            gathered,
            slot_notes,
            second_scale,
            mix_scale,
            exp_gate[0],
            exp_up[0],
            exp_down[0],
            dense_gate.T,
            dense_up.T,
            dense_down,
        ),
        out_specs=pl.BlockSpec(memory_space=pl.ANY),
        scratch_shapes=[
            pltpu.VMEM((count, slots, width), bf16),
            pltpu.SemaphoreType.DMA((2,)),
        ],
    )
    expert_out = call(
        total_kernel, shape((slots, width), bf16), *held(exchange(partial, "tp", "sums"))
    )
    returned = exchange(expert_out.reshape(groups, 4, width), "ep", "back")
    base = call(base_kernel, near((seqs, width), f32), *held(residual))
    layer_out = call(
        final_kernel, shape((seqs, width), bf16), *held(returned.reshape(slots, width), table, base)
    )
    return (layer_out, next_state)


def solution(mesh):
    in_specs = (
        P("ep", "tp"),
        P("ep", None, "tp"),
        P(),
        P(None, "tp"),
        P(None, "tp"),
        P(None, "tp"),
        P("tp", None),
        P(None, "tp"),
        P("tp"),
        P("tp", None),
        P(None, "tp"),
        P("tp"),
        P("tp"),
        P("tp"),
        P("tp"),
        P(None, "tp"),
        P(),
        P("ep", None),
        P("ep", None),
        P("ep", None, "tp"),
        P("ep", None, "tp"),
        P("ep", "tp", None),
        P(None, "tp"),
        P(None, "tp"),
        P("tp", None),
        P(),
    )
    out_specs = (P("ep", "tp"), P("ep", None, "tp"))
    return jax.shard_map(local, mesh=mesh, in_specs=in_specs, out_specs=out_specs, check_vma=False)
```

```python
import jax
import jax.numpy as jnp
from jax import lax
from jax.experimental import pallas as pl
from jax.experimental.pallas import tpu as pltpu
from jax.sharding import PartitionSpec as P


HEAD = 64
f32 = jnp.float32
bf16 = jnp.bfloat16

FIRST = {"tokens": 10, "heads": 10, "spread_out": 10, "sums": 10, "send": 23, "back": 23}

PIECE = 6

norm_eps = 1e-06
head_eps = 0.00064
key_eps = 1e-06


def dot(a, b):
    return jnp.dot(a, b, preferred_element_type=f32)


def split_dot(a, b):
    high = a.astype(bf16)
    low = (a - high.astype(f32)).astype(bf16)
    return dot(high, b) + dot(low, b)


def call(kernel, outs, *args, **kwargs):
    params = pltpu.CompilerParams(vmem_limit_bytes=12 << 20)
    return pl.pallas_call(kernel, out_shape=outs, compiler_params=params, **kwargs)(*args)


def shape(dims, dtype):
    return jax.ShapeDtypeStruct(dims, dtype)


def head_sum(x):
    first = lax.broadcasted_iota(jnp.int32, x.shape, 1) < HEAD
    left = jnp.sum(jnp.where(first, x, 0.0), axis=1, keepdims=True)
    right = jnp.sum(jnp.where(first, 0.0, x), axis=1, keepdims=True)
    return jnp.where(first, left, right)


def same_head():
    rows = lax.broadcasted_iota(jnp.int32, (2 * HEAD, 2 * HEAD), 0) // HEAD
    cols = lax.broadcasted_iota(jnp.int32, (2 * HEAD, 2 * HEAD), 1) // HEAD
    return jnp.where(rows == cols, 1.0, 0.0).astype(bf16)


def own_channel():
    rows = lax.broadcasted_iota(jnp.int32, (HEAD, 2 * HEAD), 0)
    cols = lax.broadcasted_iota(jnp.int32, (HEAD, 2 * HEAD), 1) % HEAD
    return rows == cols


def dot_t(a, b):
    return lax.dot_general(a, b, (((1,), (1,)), ((), ())), preferred_element_type=f32)


def message_kernel(place, tokens, gain, decay_down, iclr_down, out):
    rows = lax.broadcasted_iota(jnp.int32, gain.shape, 0)
    own = jnp.sum(jnp.where(rows == place[0], gain[...].astype(f32), 0.0), axis=0, keepdims=True)
    values = tokens[...].astype(f32)
    scaled = (values * own).astype(bf16)
    width = tokens.shape[1]
    low = dot_t(scaled, jnp.concatenate([decay_down[...], iclr_down[...]], axis=0))
    squares = in_three(jnp.sum(values * values, axis=1, keepdims=True))
    lanes = lax.broadcasted_iota(jnp.int32, (8, width - HEAD), 1)
    corner = jnp.zeros(lanes.shape, f32)
    for g in range(3):
        for i in range(3):
            corner = jnp.where(lanes == 3 * g + i, squares[i][8 * g : 8 * g + 8], corner)
    rest = low[:, width:]
    tail = jnp.concatenate([rest[:16], jnp.concatenate([rest[16:], corner], axis=0)], axis=1)
    whole = jnp.concatenate([scaled.astype(f32), low[:, :width], tail], axis=0).astype(bf16)
    for p in range(out.shape[0]):
        out[p] = whole


def slot_table(routes, slots, stride, first):
    top, seqs = routes.shape
    index = lax.broadcasted_iota(jnp.int32, (slots, seqs), 0)
    expert = (index // stride + first) % (slots // stride)
    matches = [jnp.where(routes[k : k + 1, :] == expert, 1.0, 0.0) for k in range(top)]
    chosen = matches[0]
    for match in matches[1:]:
        chosen = chosen + match
    earlier = lax.broadcasted_iota(jnp.int32, (seqs, seqs), 0) < lax.broadcasted_iota(
        jnp.int32, (seqs, seqs), 1
    )
    before = dot(chosen.astype(bf16), jnp.where(earlier, 1.0, 0.0).astype(bf16))
    return matches, chosen, before - (index % stride).astype(f32)


def in_three(x):
    high = x.astype(bf16).astype(f32)
    middle = (x - high).astype(bf16).astype(f32)
    return high, middle, x - high - middle


def prep_kernel(
    w_recept,
    w_key,
    w_value,
    decay_up,
    iclr_up,
    state,
    routes,
    route_weights,
    decay_base,
    iclr_base,
    key_scale,
    key_mix,
    head_gain,
    weights_out,
    ups_out,
    state_out,
    hit_out,
    notes_out,
    rows_out,
    sems,
):
    moves = [(w, weights_out.at[i]) for i, w in enumerate((w_recept, w_key, w_value))]
    moves += [(decay_up, ups_out.at[0]), (iclr_up, ups_out.at[1]), (state, state_out)]
    copies = [pltpu.make_async_copy(a, b, sems.at[i]) for i, (a, b) in enumerate(moves)]
    for copy in copies:
        copy.start()
    matches, chosen, offset = slot_table(routes, hit_out.shape[0], PIECE, FIRST["send"])
    hit_out[...] = jnp.where(offset == 0.0, chosen, 0.0).astype(bf16)
    weighted = matches[0] * route_weights[0:1, :]
    for k in range(1, len(matches)):
        weighted = weighted + matches[k] * route_weights[k : k + 1, :]
    lanes = lax.broadcasted_iota(jnp.int32, notes_out.shape, 1)
    notes = jnp.zeros(notes_out.shape, f32)
    for c in range(4):
        noted = offset == c - 4.0
        weight = jnp.sum(jnp.where(noted, weighted, 0.0), axis=1, keepdims=True)
        main = jnp.sum(jnp.where(noted, matches[0], 0.0), axis=1, keepdims=True)
        for i, column in enumerate((*in_three(weight), main)):
            notes = jnp.where(lanes == 4 * c + i, column, notes)
    rows = lax.broadcasted_iota(jnp.int32, notes_out.shape, 0)
    notes_out[...] = jnp.where(rows % PIECE == 4, notes, 0.0).astype(bf16)
    for i, row in enumerate((decay_base, iclr_base, key_scale, key_mix, head_gain)):
        rows_out[i : i + 1, :] = row[...].astype(f32)
    for copy in copies:
        copy.wait()


def gains_kernel(gain, mix, gain_out, mix_out):
    gain_out[...] = gain[...].astype(f32)
    mix_out[...] = jnp.broadcast_to(mix[...].astype(f32), mix_out.shape).astype(bf16)


def table_kernel(routes, out):
    _, chosen, offset = slot_table(routes, out.shape[0], 4, FIRST["back"])
    out[...] = jnp.where(offset == 0.0, chosen, 0.0).astype(bf16)


def mixer_in_kernel(arrived, state, weights, ups, rows, heads_out, vectors_out):
    count, _, piece = arrived.shape
    seqs = state.shape[0]
    rank = ups.shape[1]
    split = piece - rank
    decay_base, iclr_base, key_scale, key_mix, head_gain = (rows[i : i + 1, :] for i in range(5))
    first = jnp.concatenate([x[:seqs] for x in by_feature(arrived, count, "tokens")], axis=1)
    low = arrived[0, seqs:].astype(f32)
    for p in range(1, count):
        low = low + arrived[p, seqs:].astype(f32)
    tail = low[seqs:]
    lanes = lax.broadcasted_iota(jnp.int32, (8, piece), 1) - HEAD
    squares = jnp.concatenate(
        [
            jnp.sum(
                jnp.where((lanes >= 3 * g) & (lanes < 3 * g + 3), tail[8:], 0.0),
                axis=1,
                keepdims=True,
            )
            for g in range(3)
        ],
        axis=0,
    )
    scale = lax.rsqrt(squares * (1.0 / (count * piece)) + norm_eps)
    near_low = low[:seqs] * scale
    far_low = jnp.concatenate([tail[:, :HEAD], tail[:8, HEAD:]], axis=0) * scale
    decay_act = jnp.tanh(near_low[:, :rank]).astype(bf16)
    rate_near = near_low[:, rank:].astype(bf16)
    rate_far = far_low.astype(bf16)
    recept, key, value = (
        (dot(first, weights[i]) * scale).astype(bf16).astype(f32) for i in range(3)
    )
    decay_pre = -(decay_base + dot(decay_act, ups[0]))
    softplus = jnp.maximum(decay_pre, 0.0) + jnp.log1p(jnp.exp(-jnp.abs(decay_pre)))
    decay = jnp.exp(-jnp.exp(-softplus - 0.5))
    rate = jax.nn.sigmoid(iclr_base + dot(rate_near, ups[1, :split]) + dot(rate_far, ups[1, split:]))
    scaled = key * key_scale
    removal = scaled * lax.rsqrt(head_sum(scaled * scaled) + key_eps)
    written = key * (1.0 + (rate - 1.0) * key_mix)
    scaled_removal = removal * rate
    together = same_head()
    own = own_channel()

    def against(weights):
        grid = state[...] * weights[:, None, :]
        spread = split_dot(grid.reshape(seqs * HEAD, piece), together)
        return jnp.sum(jnp.where(own, spread.reshape(seqs, HEAD, piece), 0.0), axis=1)

    recall = against(removal)
    read = (
        against(decay * recept)
        - recall * head_sum(scaled_removal * recept)
        + value * head_sum(written * recept)
    )
    centered = read - head_sum(read) * (1.0 / HEAD)
    variance = head_sum(centered * centered) * (1.0 / HEAD)
    head_out = (centered * lax.rsqrt(variance + head_eps) * head_gain).astype(bf16)
    for p in range(count):
        heads_out[p] = head_out
    for i, v in enumerate((removal, decay, scaled_removal, value, written)):
        vectors_out[i] = v


def state_kernel(state, vectors, out):
    seqs, _, width = state.shape
    removal, decay, scaled_removal, value, written = (
        vectors[i][:, None, :] for i in range(5)
    )
    together = same_head()
    grid = state[...]
    recall = split_dot((grid * removal).reshape(seqs * HEAD, width), together)
    spread = jnp.where(own_channel(), value, 0.0).astype(bf16).reshape(seqs * HEAD, width)
    values = dot(spread, together)
    out[...] = (
        grid * decay
        - recall.reshape(seqs, HEAD, width) * scaled_removal
        + values.reshape(seqs, HEAD, width) * written
    )


def dispatch_kernel(heads, w_out, tokens, hit, notes, residual_out, outgoing):
    count = heads.shape[0]
    rows = jnp.concatenate([x[...] for x in by_feature(heads, count, "heads")], axis=1)
    mixed = dot(rows, w_out[...]).astype(bf16).astype(f32)
    residual = (tokens[...].astype(f32) + mixed).astype(bf16)
    residual_out[...] = residual
    outgoing[...] = (dot(hit[...], residual) + notes[...].astype(f32)).astype(bf16)


def place_in_piece(slots, size):
    slot = lax.broadcasted_iota(jnp.int32, (slots, size), 0)
    return slot % 4, lax.broadcasted_iota(jnp.int32, (slots, size), 1) - slot // 4 * PIECE


def spread_kernel(arrived, out):
    own, place = place_in_piece(out.shape[1], arrived.shape[0])
    rows = dot(jnp.where(place == own, 1.0, 0.0).astype(bf16), arrived[...]).astype(bf16)
    for p in range(out.shape[0]):
        out[p] = rows


def notes_kernel(arrived, weight_out, main_out):
    slots, width = weight_out.shape
    _, place = place_in_piece(slots, arrived.shape[0])
    notes = dot(jnp.where(place == 4, 1.0, 0.0).astype(bf16), arrived[...])
    lane = lax.broadcasted_iota(jnp.int32, (slots, width), 1)
    own = lax.broadcasted_iota(jnp.int32, (slots, width), 0) % 4
    notes = jnp.where(lane // 4 == own, notes, 0.0)
    flagged = lane % 4 == 3
    weight = jnp.sum(jnp.where(flagged, 0.0, notes), axis=1, keepdims=True)
    main = jnp.sum(jnp.where(flagged, notes, 0.0), axis=1, keepdims=True)
    weight_out[...] = jnp.broadcast_to(weight, weight_out.shape)
    main_out[...] = jnp.broadcast_to(main, main_out.shape)


def expert_kernel(
    arrived,
    weight,
    main,
    gain,
    mix,
    gate,
    up,
    down,
    dense_gate,
    dense_up,
    dense_down,
    out,
    made,
    sems,
):
    count, _, piece = arrived.shape
    pieces = [x[...].astype(f32) for x in by_feature(arrived, count, "spread_out")]
    squares = pieces[0] * pieces[0]
    for x in pieces[1:]:
        squares = squares + x * x
    scale = lax.rsqrt(
        jnp.sum(squares, axis=1, keepdims=True) * (1.0 / (count * piece)) + norm_eps
    )
    normed = [
        (x * scale * gain[p : p + 1, :]).astype(bf16) for p, x in enumerate(pieces)
    ]
    second = jnp.concatenate(normed, axis=1)
    units = gate.shape[1]
    both = dot(second, jnp.concatenate([gate[...], up[...]], axis=1))
    hidden = jax.nn.silu(both[:, :units]) * both[:, units:] * weight[...]
    small = dense_gate.shape[0]
    dense = dot_t(second, jnp.concatenate([dense_gate[...], dense_up[...], mix[...]], axis=0))
    mix_gate = jax.nn.sigmoid(dense[:, 2 * small : 2 * small + 1]) * main[:, 0:1]
    dense_hidden = jax.nn.silu(dense[:, :small]) * dense[:, small : 2 * small] * mix_gate
    joined = jnp.concatenate([hidden, dense_hidden], axis=1).astype(bf16)
    order = member_order(count, "sums")
    copies = []
    for p in range(0, count, 2):
        cols = slice(order[p] * piece, (order[p] + 2) * piece)
        block = dot(joined, jnp.concatenate([down[:, cols], dense_down[:, cols]], axis=0))
        for i in range(2):
            made[p + i] = block[:, i * piece : (i + 1) * piece].astype(bf16)
        if p % 8 == 6:
            part = pl.ds(p - 6, 8)
            copies.append(pltpu.make_async_copy(made.at[part], out.at[part], sems.at[p // 8]))
            copies[-1].start()
    for copy in copies:
        copy.wait()


def total_kernel(partial, out):
    total = partial[0].astype(f32)
    for p in range(1, partial.shape[0]):
        total = total + partial[p].astype(f32)
    turn = (FIRST["back"] - FIRST["send"]) * 4 % out.shape[0]
    if turn:
        total = jnp.concatenate([total[turn:], total[:turn]], axis=0)
    out[...] = total.astype(bf16)


def base_kernel(residual, out):
    out[...] = residual[...].astype(f32)


def final_kernel(returned, table, base, out):
    routed = lax.dot_general(
        table[...], returned[...], (((0,), (0,)), ((), ())), preferred_element_type=f32
    )
    out[...] = (base[...] + routed).astype(bf16)


def member_order(count, name):
    return [(i + FIRST[name]) % count for i in range(count)]


def by_feature(ref, count, name):
    return [ref.at[(t - FIRST[name]) % count] for t in range(count)]


def exchange(value, axis, name):
    order = member_order(lax.axis_size(axis), name)
    return lax.all_to_all(value, axis, 0, 0, tiled=True, axis_index_groups=[order])


def near(dims, dtype):
    return pltpu.VMEM(dims, dtype)


def far(*values):
    return [pltpu.with_memory_space_constraint(v, pltpu.HBM) for v in values]


def held(*values):
    return [pltpu.with_memory_space_constraint(v, pltpu.VMEM) for v in values]


def local(
    token_rows,
    prior_state,
    first_gain,
    w_recept,
    w_key,
    w_value,
    decay_down,
    decay_up,
    decay_base,
    iclr_down,
    iclr_up,
    iclr_base,
    key_scale,
    key_mix,
    head_gain,
    w_out,
    second_gain,
    routes,
    route_weights,
    exp_gate,
    exp_up,
    exp_down,
    dense_gate,
    dense_up,
    dense_down,
    dense_mix,
):
    seqs, width = token_rows.shape
    count = lax.axis_size("tp")
    groups = lax.axis_size("ep")
    slots = groups * 4
    sent_rows = groups * PIECE
    place = lax.axis_index("tp").reshape(1).astype(jnp.int32)
    row = lambda v: v.reshape(1, width)
    pieces = lambda v: v.reshape(count, width)
    in_smem = pl.BlockSpec(memory_space=pltpu.SMEM)
    in_vmem = pl.BlockSpec(memory_space=pltpu.VMEM)
    message = call(
        message_kernel,
        shape((count, 2 * seqs + 16, width), bf16),
        place,
        *far(token_rows, pieces(first_gain), decay_down.T, iclr_down.T),
        in_specs=[in_smem] + [in_vmem] * 4,
    )
    arrived = exchange(message, "tp", "tokens")
    weights, ups, state, hit, notes, rows_of = call(
        prep_kernel,
        (
            near((3, *w_key.shape), bf16),
            near((2, *decay_up.shape), bf16),
            near(prior_state.shape, f32),
            near((sent_rows, seqs), bf16),
            near((sent_rows, width), bf16),
            near((8, width), f32),
        ),
        *far(
            w_recept,
            w_key,
            w_value,
            decay_up,
            iclr_up,
            prior_state,
            routes.T,
            route_weights.T,
            row(decay_base),
            row(iclr_base),
            row(key_scale),
            row(key_mix),
            row(head_gain),
        ),
        in_specs=[pl.BlockSpec(memory_space=pl.ANY)] * 6 + [in_vmem] * 7,
        scratch_shapes=[pltpu.SemaphoreType.DMA((6,))],
    )
    heads, vectors = call(
        mixer_in_kernel,
        (near((count, seqs, width), bf16), near((5, seqs, width), f32)),
        *held(arrived, state, weights, ups, rows_of),
    )
    heads_all = exchange(heads, "tp", "heads")
    block = 8
    next_state = call(
        state_kernel,
        shape(prior_state.shape, f32),
        *far(prior_state),
        *held(vectors),
        grid=(seqs // block,),
        in_specs=[
            pl.BlockSpec((block, HEAD, width), lambda i: (i, 0, 0)),
            pl.BlockSpec((5, block, width), lambda i: (0, i, 0)),
        ],
        out_specs=pl.BlockSpec((block, HEAD, width), lambda i: (i, 0, 0)),
    )
    residual, outgoing = call(
        dispatch_kernel,
        (near((seqs, width), bf16), shape((sent_rows, width), bf16)),
        *held(heads_all, w_out, token_rows, hit, notes),
    )
    sent = exchange(outgoing.reshape(groups, PIECE // 2, 2, width), "ep", "send")
    second_scale, mix_scale = call(
        gains_kernel,
        (near((count, width), f32), near((8, count * width), bf16)),
        *far(pieces(second_gain), dense_mix.reshape(1, count * width)),
    )
    sent = sent.reshape(sent_rows, width)
    rows = call(spread_kernel, shape((count, slots, width), bf16), *held(sent))
    gathered = exchange(rows, "tp", "spread_out")
    table = call(table_kernel, near((slots, seqs), bf16), *far(routes.T))
    slot_weight, slot_main = call(
        notes_kernel, (near((slots, width), f32), near((slots, width), f32)), *held(sent)
    )
    partial = call(
        expert_kernel,
        shape((count, slots, width), bf16),
        *held(
            gathered,
            slot_weight,
            slot_main,
            second_scale,
            mix_scale,
            exp_gate[0],
            exp_up[0],
            exp_down[0],
            dense_gate.T,
            dense_up.T,
            dense_down,
        ),
        out_specs=pl.BlockSpec(memory_space=pl.ANY),
        scratch_shapes=[
            pltpu.VMEM((count, slots, width), bf16),
            pltpu.SemaphoreType.DMA((2,)),
        ],
    )
    expert_out = call(
        total_kernel, shape((slots, width), bf16), *held(exchange(partial, "tp", "sums"))
    )
    returned = exchange(expert_out.reshape(groups, 4, width), "ep", "back")
    base = call(base_kernel, near((seqs, width), f32), *held(residual))
    layer_out = call(
        final_kernel, shape((seqs, width), bf16), *held(returned.reshape(slots, width), table, base)
    )
    return (layer_out, next_state)


def solution(mesh):
    in_specs = (
        P("ep", "tp"),
        P("ep", None, "tp"),
        P(),
        P(None, "tp"),
        P(None, "tp"),
        P(None, "tp"),
        P("tp", None),
        P(None, "tp"),
        P("tp"),
        P("tp", None),
        P(None, "tp"),
        P("tp"),
        P("tp"),
        P("tp"),
        P("tp"),
        P(None, "tp"),
        P(),
        P("ep", None),
        P("ep", None),
        P("ep", None, "tp"),
        P("ep", None, "tp"),
        P("ep", "tp", None),
        P(None, "tp"),
        P(None, "tp"),
        P("tp", None),
        P(),
    )
    out_specs = (P("ep", "tp"), P("ep", None, "tp"))
    return jax.shard_map(local, mesh=mesh, in_specs=in_specs, out_specs=out_specs, check_vma=False)
```
